32 devices in a mesh: sp: 8 (over z, core), tp: 4 (over y, x).
Axes of the slice: x: 2, y: 2, z: 4, core: 2. Of those that a mesh axis runs over, the one named last changes fastest.
Arguments:
- stream: bfloat16 [2048, 1024], P('tp', 'sp')
- values_in: bfloat16 [1024, 1024], P('tp', 'sp'), may hold values from -6 to 6
- in_gate: bfloat16 [1024, 1024], P('tp', 'sp'), may hold values from -6 to 6
- out_gate: bfloat16 [1024, 1024], P('tp', 'sp'), may hold values from -6 to 6
- documents: int32 [1024], P('sp'), may hold values from 0 to 15, never falling along the last dimension, each value on 1 to 256 neighbouring positions
- conv_taps: float32 [3, 1024], P(None, 'tp'), may hold values from -3.5 to 3.5
- head_gain: float32 [1024], P('tp'), may hold values from 0.1 to 1.9
- mix_weight: bfloat16 [1024, 2048], P('tp'), may hold values from -0.25 to 0.25
- norm_gain: float32 [2048], P('tp'), may hold values from 0.1 to 1.9
- routes: int32 [1024, 4], P('sp'), may hold values from 0 to 7, all different within a row; in each aligned block of 128 rows (0 to 127, 128 to 255, ...) at most 96 rows name the same one
- route_weight: float32 [1024, 4], P('sp'), may hold values from 0.2 to 1
- expert_gate: bfloat16 [8, 2048, 2048], P('sp', None, 'tp'), may hold values from -0.125 to 0.125
- expert_up: bfloat16 [8, 2048, 2048], P('sp', None, 'tp'), may hold values from -0.125 to 0.125
- expert_down: bfloat16 [8, 2048, 2048], P('sp', None, 'tp'), may hold values from -0.125 to 0.125
- shared_gate: bfloat16 [2048, 2048], P(None, 'tp'), may hold values from -0.125 to 0.125
- shared_up: bfloat16 [2048, 2048], P(None, 'tp'), may hold values from -0.125 to 0.125
- shared_down: bfloat16 [2048, 2048], P('tp'), may hold values from -0.1875 to 0.1875
Outputs:
- layer_out: bfloat16 [2048, 1024], P('tp', 'sp')
The draws below stay inside these ranges and needn't reach their ends.
Inputs may be any that keep to these rules, and one draw needn't show every extreme that they name: `routes`: each row names 4 different experts. In each aligned block of 128 rows no expert is named by more than 96 rows, a bound that some block reaches. `documents`: document numbers never fall along the positions; each document has 1 to 256 positions, and one has exactly that many.
All inputs are finite; a program needn't handle non-finite values.
Results may differ from the reference program's by a relative error of at most 0.015.
Values may be sent and summed in bfloat16 or wider, within the bound.
A program may use at most 64 MiB of HBM per device.

```python
import math
import jax
import jax.numpy as jnp
import numpy as np
from jax import lax

D = 2048
HEADS = 16
HEAD = 64
CW = 1024
FE = 2048
FS = 2048
TOP_K = 4
TOK_DEV = 128
TOKENS = 1024
EXPERTS = 8
CAP = 96
N_SP = 8
N_TP = 4


def draw_stream(key, part):
    first = jax.random.fold_in(jax.random.fold_in(key, 11), 0)
    feature_scale = 0.5 * 4.0 ** (jnp.arange(D, dtype=jnp.float32) / D)
    base = jax.random.normal(first, (D, TOKENS), jnp.float32)
    return (base * feature_scale[:, None]).astype(jnp.bfloat16)


def with_spikes(entries, key, source, target, blocks, factor):
    owner, partner = [(jnp.arange(entries.shape[position]) // (entries.shape[position] // blocks)).reshape([-1 if axis == position else 1 for axis in range(entries.ndim)]) for position in (source, target)]
    chosen = jax.random.permutation(key, blocks)[partner]
    strong = (owner == chosen) | (owner == (partner + blocks // 2) % blocks)
    return jnp.where(strong, factor * entries, entries)


def steps_of(own_key, shape, pieces, low, high):
    factor_of = 1.0
    for dim, blocks in pieces:
        heights = jax.random.uniform(jax.random.fold_in(jax.random.fold_in(own_key, 6), dim), (blocks,), jnp.float32, low / len(pieces), high / len(pieces))
        factor_of = factor_of * jnp.repeat(jnp.exp(heights), shape[dim] // blocks).reshape((-1,) + (1,) * (len(shape) - 1 - dim))
    return factor_of


def profile(number_of, total, reach, slope):
    weights = [(1 << 20) // math.isqrt(rank ** slope) + 1 for rank in range(2, number_of + 1)]
    spare, counts = total - reach - (number_of - 1), [1] * (number_of - 1)
    while spare > 0:
        free = [i for i in range(number_of - 1) if counts[i] < reach]
        pool, budget = sum([weights[i] for i in free]), spare
        for i in free:
            addition = min(reach - counts[i], max(1, budget * weights[i] // pool), spare)
            counts[i] = counts[i] + addition
            spare = spare - addition
    return np.array([reach] + counts)


def uneven_parts(own_key, number_of, total, most, lean):
    if number_of == 2:
        one = jax.random.randint(own_key, (), max(1, total - most), min(most, total - 1) + 1)
        return jnp.stack([one, total - one])
    lengths = jnp.asarray(profile(number_of, total, most, lean), jnp.int32)
    twos = (number_of - 1) // 2
    donor, receiver = lengths[1:1 + 2 * twos:2], lengths[2:2 + 2 * twos:2]
    room = jnp.minimum(donor - 1, most - receiver)
    passed = jax.random.randint(jax.random.fold_in(own_key, 1), (twos,), 0, 1 << 20) % (room + 1)
    lengths = lengths.at[1:1 + 2 * twos:2].set(donor - passed).at[2:2 + 2 * twos:2].set(receiver + passed)
    return lengths[jax.random.permutation(jax.random.fold_in(own_key, 2), number_of)]


def deal_out(stream_key, own, number, rows, amount, top, reach, lean):
    ranking = jax.random.permutation(stream_key, amount)
    heavy_load, usual = portions_of(amount, rows * top, reach, lean, True), portions_of(amount, rows * top, reach, lean, False)
    places = jnp.arange(amount)

    def named(lengths, turn):
        used = int((lengths > 0).sum())
        fixed = max(1, used // 4)
        passed = fixed + (places - fixed + turn * (used - fixed)) % max(1, amount - fixed)
        return jnp.zeros((amount,), jnp.int32).at[ranking[jnp.where(places < fixed, places, passed)]].set(jnp.asarray(lengths, jnp.int32))

    lengths = jnp.where(number % 4 == 0, named(heavy_load, number // 4), named(usual, number - number // 4 - 1))
    mixed = jax.random.permutation(jax.random.fold_in(own, 3), amount)
    source_of, taker = mixed[0:amount // 2 * 2:2], mixed[1:amount // 2 * 2:2]
    room = jnp.minimum(lengths[source_of] - 1, reach - lengths[taker]) // 2
    room = jnp.where((source_of == ranking[0]) | (taker == ranking[0]) | (lengths[taker] == 0), 0, jnp.maximum(room, 0))
    passed = jax.random.randint(jax.random.fold_in(own, 4), (amount // 2,), 0, 1 << 20) % (room + 1)
    lengths = lengths.at[source_of].add(-passed).at[taker].add(passed)
    items = jnp.searchsorted(jnp.cumsum(lengths), jnp.arange(rows * top), side="right").astype(jnp.int32)
    listing = items.reshape(top, rows).T
    listing = listing[jax.random.permutation(jax.random.fold_in(own, 1), rows)]
    turn = jax.random.randint(jax.random.fold_in(own, 2), (rows, 1), 0, top)
    return jnp.take_along_axis(listing, (jnp.arange(top)[None, :] + turn) % top, axis=1)


def portions_of(amount, total, bound, skew, full):
    loads = [(1 << 20) // math.isqrt(standing ** skew) + 1 for standing in range(1, amount + 1)]
    largest = bound if full else min(bound, max(-(-total // amount), total * loads[0] // sum(loads)))
    least = 1 if total - largest >= amount - 1 else 0
    given, rest = [largest] + [least] * (amount - 1), total - largest - least * (amount - 1)
    while rest > 0:
        movable = [i for i in range(1, amount) if given[i] < largest] or [i for i in range(1, amount) if given[i] < bound]
        mass, budget = sum([loads[i] for i in movable]), rest
        for i in movable:
            more = min(bound - given[i], max(1, budget * loads[i] // mass), rest)
            given[i] = given[i] + more
            rest = rest - more
    return np.array(given)


def noise(own_key, extent, scale, bound, cuts=(), kind=jnp.bfloat16):
    array = jax.random.normal(own_key, extent, jnp.float32) * scale
    if len(cuts) > 0:
        array = steps_of(own_key, extent, cuts, -0.22, 0.18) * array
    return jnp.clip(array, min=-bound, max=bound).astype(kind)


def bell_draw_with(own_key, dims, scale, most, cuts, heavy, kind=jnp.bfloat16):
    result = scale * jax.random.normal(own_key, dims, jnp.float32)
    if cuts:
        result = result * steps_of(own_key, dims, cuts, -0.22, 0.18)
    return jnp.clip(with_spikes(result, jax.random.fold_in(own_key, 3), *heavy), -most, most).astype(kind)


def setup_inputs(seed: int = 0) -> dict:
    seeds = jax.random.split(jax.random.key(seed), 18)
    stream = draw_stream(jax.random.fold_in(seeds[17], 71), 0)
    values_in = noise(seeds[1], (CW, TOKENS), 1.0, 6.0, ((0, 4), (1, 8)))
    in_gate = noise(seeds[2], (CW, TOKENS), 1.0, 6.0, ((0, 4), (1, 8)))
    out_gate = noise(seeds[3], (CW, TOKENS), 1.0, 6.0, ((0, 4), (1, 8)))
    documents = jnp.searchsorted(jnp.cumsum(uneven_parts(seeds[4], 2 * N_SP, TOKENS, 2 * TOK_DEV, 1)), jnp.arange(TOKENS), side="right").astype(jnp.int32)
    conv_taps = noise(seeds[5], (3, CW), 3 ** -0.5, 3.5, ((1, 4),), jnp.float32)
    head_gain = jnp.clip(1.0 + 0.18 * jax.random.normal(seeds[6], (CW,), jnp.float32), 0.1, 1.9)
    mix_weight = bell_draw_with(seeds[7], (CW, D), CW ** -0.5, 0.25, ((0, 4),), (0, 1, 4, 2.0))
    norm_gain = jnp.clip(1.0 + 0.18 * jax.random.normal(seeds[8], (D,), jnp.float32), 0.1, 1.9)
    routes_keys = jax.random.split(jax.random.fold_in(seeds[9], 1), TOKENS // TOK_DEV)
    routes_turns = jax.random.permutation(jax.random.fold_in(seeds[9], 3), TOKENS // TOK_DEV)
    routes = jax.vmap(lambda own, number: deal_out(jax.random.fold_in(seeds[9], 2), own, number, TOK_DEV, EXPERTS, TOP_K, CAP, 1))(routes_keys, routes_turns).reshape((TOKENS, TOP_K))
    route_weight = jnp.clip(0.2 + 0.8 * jax.random.uniform(seeds[10], (TOKENS, TOP_K), jnp.float32) ** steps_of(seeds[10], (TOKENS, TOP_K), ((0, 8),), -0.2, 0.2), 0.2, 1.0)
    expert_gate = noise(seeds[11], (EXPERTS, D, FE), D ** -0.5, 0.125, ((0, 8), (2, 4)))
    expert_up = noise(seeds[12], (EXPERTS, D, FE), D ** -0.5, 0.125, ((0, 8), (2, 4)))
    expert_down = noise(seeds[13], (EXPERTS, FE, D), FE ** -0.5, 0.125, ((0, 8), (2, 4)))
    shared_gate = noise(seeds[14], (D, FS), D ** -0.5, 0.125, ((1, 4),))
    shared_up = noise(seeds[15], (D, FS), D ** -0.5, 0.125, ((1, 4),))
    shared_down = bell_draw_with(seeds[16], (FS, D), FS ** -0.5, 0.1875, ((0, 4),), (0, 1, 4, 2.0))
    return {"stream": stream, "values_in": values_in, "in_gate": in_gate, "out_gate": out_gate, "documents": documents, "conv_taps": conv_taps, "head_gain": head_gain, "mix_weight": mix_weight, "norm_gain": norm_gain, "routes": routes, "route_weight": route_weight, "expert_gate": expert_gate, "expert_up": expert_up, "expert_down": expert_down, "shared_gate": shared_gate, "shared_up": shared_up, "shared_down": shared_down}


epsilon = 1e-06

def rounded(value):
    return lax.optimization_barrier(value.astype(jnp.bfloat16)).astype(jnp.float32)

def block_sum(left, right, parts):
    width = left.shape[1] // parts
    running = jnp.zeros((left.shape[0], right.shape[1]), jnp.float32)
    for block in range(parts):
        term = jnp.dot(left[:, block * width:(block + 1) * width], right[block * width:(block + 1) * width], preferred_element_type=jnp.float32)
        running = running + rounded(term)
    return running

def reference(stream, values_in, in_gate, out_gate, documents, conv_taps, head_gain, mix_weight, norm_gain, routes, route_weight, expert_gate, expert_up, expert_down, shared_gate, shared_up, shared_down):
    product = values_in.astype(jnp.float32) * in_gate.astype(jnp.float32)
    length = product.shape[1]
    padded = jnp.pad(product, ((0, 0), (2, 0)))
    doc_ids = jnp.pad(documents, (2, 0), constant_values=-1)
    convolved = jnp.zeros(product.shape, jnp.float32)
    for offset in range(3):
        same_doc = (doc_ids[offset:offset + length] == documents).astype(jnp.float32)
        convolved = convolved + conv_taps[offset][:, None] * padded[:, offset:offset + length] * same_doc[None, :]
    mixed = out_gate.astype(jnp.float32) * convolved
    heads = mixed.reshape(HEADS, HEAD, length)
    heads = heads * lax.rsqrt(lax.optimization_barrier(jnp.mean(heads * heads, axis=1, keepdims=True)) + epsilon)
    normed_heads = (heads.reshape(CW, length) * head_gain[:, None]).astype(jnp.bfloat16)
    mixer = block_sum(normed_heads.T, mix_weight, N_TP)
    hidden_state = stream.astype(jnp.float32).T + mixer
    normed = (hidden_state * lax.rsqrt(lax.optimization_barrier(jnp.mean(hidden_state * hidden_state, axis=1, keepdims=True)) + epsilon) * norm_gain[None, :]).astype(jnp.bfloat16)
    shared_mid = (jax.nn.silu(jnp.dot(normed, shared_gate, preferred_element_type=jnp.float32)) * jnp.dot(normed, shared_up, preferred_element_type=jnp.float32)).astype(jnp.bfloat16)
    shared = block_sum(shared_mid, shared_down, N_TP)
    groups = TOKENS // TOK_DEV
    flat_routes = routes.reshape(groups, TOK_DEV * TOP_K)
    onehot = (flat_routes[:, :, None] == jnp.arange(EXPERTS, dtype=jnp.int32)[None, None, :]).astype(jnp.int32)
    earlier = jnp.cumsum(onehot, axis=1) - onehot
    slot = lax.optimization_barrier(jnp.sum(earlier * onehot, axis=2))
    column = (jnp.arange(groups, dtype=jnp.int32)[:, None] * CAP + slot).reshape(-1).astype(jnp.int32)
    owner = (jnp.arange(TOKENS * TOP_K, dtype=jnp.int32) // TOP_K).astype(jnp.int32)
    chosen = flat_routes.reshape(-1)
    table = jnp.zeros((EXPERTS, groups * CAP), jnp.int32).at[chosen, column].set(owner)
    filled = jnp.zeros((EXPERTS, groups * CAP), jnp.bfloat16).at[chosen, column].set(1.0)

    def expert(number):
        rows = normed[table[number]] * filled[number][:, None]
        gate = jnp.dot(rows, expert_gate[number], preferred_element_type=jnp.float32)
        upward = jnp.dot(rows, expert_up[number], preferred_element_type=jnp.float32)
        middle = (jax.nn.silu(gate) * upward).astype(jnp.bfloat16)
        return jnp.dot(middle, expert_down[number], preferred_element_type=jnp.float32).astype(jnp.bfloat16)
    outputs = lax.map(expert, jnp.arange(EXPERTS, dtype=jnp.int32))
    picked = outputs[chosen, column].astype(jnp.float32).reshape(TOKENS, TOP_K, D)
    routed = lax.optimization_barrier(jnp.sum(picked * route_weight[:, :, None], axis=1))
    return (hidden_state + shared + routed).astype(jnp.bfloat16).T
```

```python
import functools

import jax
import jax.numpy as jnp
from jax import lax
from jax.experimental import pallas as pl
from jax.experimental.pallas import tpu as pltpu
from jax.sharding import PartitionSpec as P

HEAD = 64
CORES = 2
CHUNKS = 4
SUB = 8
epsilon = 1e-06
MESH = pl.DeviceIdType.MESH
F32 = jnp.float32
BF16 = jnp.bfloat16


def flipped(index, mask):
    bit = 1
    out = index
    while bit <= mask:
        if mask & bit:
            out = out + bit - 2 * bit * lax.rem(lax.div(index, bit), 2)
        bit *= 2
    return out


def dot(left, right):
    return jnp.dot(left, right, preferred_element_type=F32)


def silu(value):
    return value / (1.0 + jnp.exp(-value))


def column_of(row, width):
    return jnp.broadcast_to(row, (width, row.shape[1])).T


def kernel(
    n_sp, n_tp,
    stream, values_in, in_gate, out_gate, documents, conv_taps, head_gain, mix_weight,
    norm_gain, routes, route_weight, expert_gate, expert_up, expert_down,
    shared_gate, shared_up, shared_down,
    out,
    mix_w, gate_w, up_w, sgate_w, sup_w, sdown_w, down_w,
    tail_s, prev_r, prev_docs, mix_s, mix_r, hidden_v, x_all, ss_s, ss_r, meta_r,
    mid_v, shared_v, acc_v, pr_s, pr_r, rs_s, rs_r, zr_s, zr_r,
    load_sem, local_sem, halo_send, halo_recv, mix_send, mix_recv, ss_send, ss_recv,
    meta_send, meta_recv, x_recv, xs_tp, xs_z, xs_p, wd_send, wd_recv,
    pr_send, pr_recv, rs_send, rs_recv, zr_send, zr_recv,
):
    sp = lax.axis_index("sp")
    tp = lax.axis_index("tp")
    z = lax.div(sp, CORES)
    core = lax.rem(sp, CORES)
    n_z = n_sp // CORES
    feats, pos = stream.shape
    chans = values_in.shape[0]
    width = feats * n_tp
    hid = gate_w.shape[1]
    partner = {"sp": z * CORES + 1 - core}
    peers = [flipped(tp, d) for d in range(1, n_tp)]
    pending = []

    def send(src, dst, ssem, rsem, device):
        copy = pltpu.make_async_remote_copy(
            src_ref=src, dst_ref=dst, send_sem=ssem, recv_sem=rsem,
            device_id=device, device_id_type=MESH,
        )
        copy.start()
        pending.append(copy)

    def arrived(dst, rsem):
        pltpu.make_async_remote_copy(
            src_ref=dst, dst_ref=dst, send_sem=rsem, recv_sem=rsem,
            device_id=partner, device_id_type=MESH,
        ).wait_recv()

    loads = [
        pltpu.make_async_copy(src, dst, load_sem.at[i])
        for i, (src, dst) in enumerate([
            (mix_weight, mix_w), (shared_gate, sgate_w), (shared_up, sup_w),
            (shared_down, sdown_w), (expert_gate.at[0], gate_w), (expert_up.at[0], up_w),
        ])
    ]
    loads[0].start()

    barrier = pltpu.get_barrier_semaphore()
    for peer in peers:
        pl.semaphore_signal(barrier, inc=1, device_id={"tp": peer}, device_id_type=MESH)
    for d in range(1, n_sp):
        pl.semaphore_signal(
            barrier, inc=1, device_id={"sp": lax.rem(sp + d, n_sp)}, device_id_type=MESH
        )
    pl.semaphore_wait(barrier, n_tp - 1 + n_sp - 1)

    product = values_in[...].astype(F32) * in_gate[...].astype(F32)
    tail_s[...] = product.T[pos - SUB:, :]
    after = {"sp": lax.rem(sp + 1, n_sp)}
    send(tail_s, prev_r.at[pl.ds(pos - SUB, SUB)], halo_send.at[0], halo_recv.at[0], after)
    send(documents, prev_docs, halo_send.at[1], halo_recv.at[1], after)

    rows = hid // CHUNKS

    def send_down(chunk):
        for d, peer in enumerate(peers):
            start = pl.multiple_of(peer * hid + chunk * rows, rows)
            send(
                expert_down.at[0, pl.ds(start, rows), :],
                down_w.at[tp, pl.ds(chunk * rows, rows), :],
                wd_send.at[d, chunk], wd_recv.at[tp, chunk], {"tp": peer},
            )

    send_down(0)
    own_down = pltpu.make_async_copy(
        expert_down.at[0, pl.ds(pl.multiple_of(tp * hid, hid), hid), :], down_w.at[tp], local_sem
    )
    for load in loads[1:]:
        load.start()
    own_down.start()

    named = routes[...]
    weights = route_weight[...]
    meta_rows = meta_r.shape[1]
    lane = lax.broadcasted_iota(jnp.int32, (pos, pos), 1)
    table = jnp.zeros((pos, pos), F32)
    for k in range(routes.shape[1]):
        table = table + jnp.where(lane == named[:, k:k + 1], weights[:, k:k + 1], 0.0)
    table = table.T[:meta_rows]
    taps = [column_of(conv_taps[j:j + 1, :], pos) for j in range(3)]
    stream_t = stream[...].astype(F32).T

    prev_r[: pos - SUB, :] = jnp.zeros((pos - SUB, chans), F32)
    arrived(prev_r.at[pl.ds(pos - SUB, SUB)], halo_recv.at[0])
    arrived(prev_docs, halo_recv.at[1])
    before = prev_r[...].T
    docs = documents[...]
    docs_before = jnp.where(sp > 0, prev_docs[...], -1)
    lane_c = lax.broadcasted_iota(jnp.int32, (chans, pos), 1)
    lane_1 = lax.broadcasted_iota(jnp.int32, (1, pos), 1)
    convolved = taps[2] * product
    for shift in (1, 2):
        moved = jnp.where(lane_c < shift, pltpu.roll(before, shift, 1), pltpu.roll(product, shift, 1))
        ids = jnp.where(lane_1 < shift, pltpu.roll(docs_before, shift, 1), pltpu.roll(docs, shift, 1))
        convolved = convolved + jnp.where(ids == docs, taps[2 - shift] * moved, 0.0)
    mixed = out_gate[...].astype(F32) * convolved
    heads = mixed.reshape(chans // HEAD, HEAD, pos)
    heads = heads * lax.rsqrt(jnp.mean(heads * heads, axis=1, keepdims=True) + epsilon)
    heads_t = (heads.reshape(chans, pos).T * head_gain[...]).astype(BF16)

    loads[0].wait()
    for b, peer in enumerate(peers + [tp]):
        cols = pl.ds(pl.multiple_of(peer * feats, feats), feats)
        mix_s[b] = dot(heads_t, mix_w[:, cols]).astype(BF16)
        if b < n_tp - 1:
            send(mix_s.at[b], mix_r.at[b], mix_send.at[b], mix_recv.at[b], {"tp": peer})
    send_down(1)

    hidden = stream_t + mix_s[n_tp - 1].astype(F32)
    for b in range(n_tp - 1):
        arrived(mix_r.at[b], mix_recv.at[b])
        hidden = hidden + mix_r[b].astype(F32)
    hidden_v[...] = hidden
    x_all[sp, tp] = (hidden * norm_gain[...]).astype(BF16)
    own = x_all.at[sp, tp]
    for d in range(1, n_z):
        send(own, own, xs_z.at[d], x_recv.at[sp, tp],
             {"sp": lax.rem(z + d, n_z) * CORES + core})
    for b, peer in enumerate(peers):
        send(own, own, xs_tp.at[0, b], x_recv.at[sp, tp], {"tp": peer})
    send(own, own, xs_p.at[0, 0], x_recv.at[sp, tp], partner)

    squares = jnp.sum(hidden * hidden, axis=1, keepdims=True)
    row = jnp.broadcast_to(squares, (pos, pos)).T[:SUB]
    ss_s[...] = row
    for b, peer in enumerate(peers):
        send(ss_s, ss_r.at[b], ss_send.at[b], ss_recv.at[b], {"tp": peer})
    send_down(2)
    for b in range(n_tp - 1):
        arrived(ss_r.at[b], ss_recv.at[b])
        row = row + ss_r[b]
    scale = lax.rsqrt(row[:1] / width + epsilon)
    at_row = lax.broadcasted_iota(jnp.int32, (meta_rows, pos), 0)
    meta_r[sp] = jnp.where(at_row == meta_rows - 1, scale, table)
    for d in range(1, n_sp):
        send(meta_r.at[sp], meta_r.at[sp], meta_send.at[d], meta_recv.at[sp],
             {"sp": lax.rem(sp + d, n_sp)})

    def forward(slot, group):
        for b, peer in enumerate(peers):
            block = x_all.at[group, peer]
            arrived(block, x_recv.at[group, peer])
            send(block, block, xs_p.at[slot, b + 1], x_recv.at[group, peer], partner)

    forward(0, sp)

    loads[1].wait()
    loads[2].wait()
    scale_own = column_of(scale, pos)[:, :1]
    gate = jnp.zeros((pos, hid), F32)
    upward = jnp.zeros((pos, hid), F32)
    for b in range(n_tp):
        block = x_all[sp, b]
        gate = gate + dot(block, sgate_w[b * feats:(b + 1) * feats, :])
        upward = upward + dot(block, sup_w[b * feats:(b + 1) * feats, :])
    shared_mid = (silu(gate * scale_own) * (upward * scale_own)).astype(BF16)
    loads[3].wait()
    shared_v[...] = dot(shared_mid, sdown_w[...])

    for d in range(1, n_z):
        group = lax.rem(z + n_z - d, n_z) * CORES + core
        block = x_all.at[group, tp]
        arrived(block, x_recv.at[group, tp])
        for b, peer in enumerate(peers):
            send(block, block, xs_tp.at[d, b], x_recv.at[group, tp], {"tp": peer})
        send(block, block, xs_p.at[d, 0], x_recv.at[group, tp], partner)
    for chunk in range(3, CHUNKS):
        send_down(chunk)

    loads[4].wait()
    loads[5].wait()
    for d in range(n_z):
        layer = lax.rem(z + n_z - d, n_z)
        mine = layer * CORES + core
        other = layer * CORES + 1 - core
        if d > 0:
            forward(d, mine)
            arrived(meta_r.at[mine], meta_recv.at[mine])
        arrived(meta_r.at[other], meta_recv.at[other])
        for b in range(n_tp):
            arrived(x_all.at[other, b], x_recv.at[other, b])
        gate = jnp.zeros((CORES * pos, hid), F32)
        upward = jnp.zeros((CORES * pos, hid), F32)
        for b in range(n_tp):
            block = x_all[pl.ds(layer * CORES, CORES), b].reshape(CORES * pos, feats)
            gate = gate + dot(block, gate_w[b * feats:(b + 1) * feats, :])
            upward = upward + dot(block, up_w[b * feats:(b + 1) * feats, :])
        scales = jnp.concatenate([
            column_of(meta_r[layer * CORES + i, meta_rows - 1:, :], pos)[:, :1]
            for i in range(CORES)
        ], axis=0)
        mid_v[layer] = (silu(gate * scales) * (upward * scales)).astype(BF16)

    own_down.wait()
    for peer in peers:
        for chunk in range(CHUNKS):
            arrived(down_w.at[peer, pl.ds(chunk * rows, rows), :], wd_recv.at[peer, chunk])

    order = list(range(1, n_z)) + [0]
    totals = {}

    def layer_of(step):
        return lax.rem(z + order[step], n_z)

    def multiply(step):
        layer = layer_of(step)
        for half in range(2):
            group = layer * CORES + (1 - core if half == 0 else core)
            weight = column_of(meta_r[group, pl.ds(sp, 1), :], pos)[:, :1]
            start = pl.multiple_of((group - layer * CORES) * pos, pos)
            middle = mid_v[layer, pl.ds(start, pos), :]
            for b in range(n_tp):
                term = dot(middle, down_w[b]) * weight
                if half == 0:
                    pr_s[step, b] = term.astype(BF16)
                else:
                    acc_v[step % 2, b] = term
            if half == 0:
                send(pr_s.at[step], pr_r.at[step], pr_send.at[step], pr_recv.at[step], partner)

    def spread(step):
        arrived(pr_r.at[step], pr_recv.at[step])
        for b, peer in enumerate(peers + [tp]):
            term = acc_v[step % 2, peer] + pr_r[step, peer].astype(F32)
            if order[step] == 0:
                cols = pl.ds(pl.multiple_of(peer * feats, feats), feats)
                term = term + shared_v[:, cols]
            rs_s[step, b] = term.astype(BF16)
            if b < n_tp - 1:
                send(rs_s.at[step, b], rs_r.at[step, b], rs_send.at[step, b],
                     rs_recv.at[step, b], {"tp": peer})

    def gathered(step):
        total = rs_s[step, n_tp - 1].astype(F32)
        for b in range(n_tp - 1):
            arrived(rs_r.at[step, b], rs_recv.at[step, b])
            total = total + rs_r[step, b].astype(F32)
        d = order[step]
        if d == 0:
            totals[0] = total
        else:
            zr_s[d] = total.astype(BF16)
            send(zr_s.at[d], zr_r.at[d], zr_send.at[d], zr_recv.at[d],
                 {"sp": layer_of(step) * CORES + core})

    for step in range(n_z + 2):
        if step < n_z:
            multiply(step)
        if 0 <= step - 1 < n_z:
            spread(step - 1)
        if 0 <= step - 2 < n_z:
            gathered(step - 2)

    result = hidden_v[...] + totals[0]
    for d in range(1, n_z):
        arrived(zr_r.at[d], zr_recv.at[d])
        result = result + zr_r[d].astype(F32)
    out[...] = result.T.astype(BF16)
    for copy in pending:
        copy.wait_send()


def local(n_sp, n_tp, *args):
    (stream, values_in, in_gate, out_gate, documents, conv_taps, head_gain, mix_weight,
     norm_gain, routes, route_weight, expert_gate, expert_up, expert_down,
     shared_gate, shared_up, shared_down) = args
    feats, pos = stream.shape
    chans = values_in.shape[0]
    width = feats * n_tp
    hid = expert_gate.shape[2]
    n_z = n_sp // CORES
    meta_rows = -(-(n_sp + 1) // SUB) * SUB
    vmem = pl.BlockSpec(memory_space=pltpu.VMEM)
    anywhere = pl.BlockSpec(memory_space=pl.ANY)
    dma = pltpu.SemaphoreType.DMA
    scratch = [
        pltpu.VMEM((chans, width), BF16),
        pltpu.VMEM((width, hid), BF16),
        pltpu.VMEM((width, hid), BF16),
        pltpu.VMEM((width, hid), BF16),
        pltpu.VMEM((width, hid), BF16),
        pltpu.VMEM((hid, width), BF16),
        pltpu.VMEM((n_tp, hid, feats), BF16),
        pltpu.VMEM((SUB, chans), F32),
        pltpu.VMEM((pos, chans), F32),
        pltpu.VMEM((1, pos), jnp.int32),
        pltpu.VMEM((n_tp, pos, feats), BF16),
        pltpu.VMEM((n_tp, pos, feats), BF16),
        pltpu.VMEM((pos, feats), F32),
        pltpu.VMEM((n_sp, n_tp, pos, feats), BF16),
        pltpu.VMEM((SUB, pos), F32),
        pltpu.VMEM((n_tp, SUB, pos), F32),
        pltpu.VMEM((n_sp, meta_rows, pos), F32),
        pltpu.VMEM((n_z, CORES * pos, hid), BF16),
        pltpu.VMEM((pos, width), F32),
        pltpu.VMEM((2, n_tp, pos, feats), F32),
        pltpu.VMEM((n_z, n_tp, pos, feats), BF16),
        pltpu.VMEM((n_z, n_tp, pos, feats), BF16),
        pltpu.VMEM((n_z, n_tp, pos, feats), BF16),
        pltpu.VMEM((n_z, n_tp, pos, feats), BF16),
        pltpu.VMEM((n_z, pos, feats), BF16),
        pltpu.VMEM((n_z, pos, feats), BF16),
        dma((6,)), dma,
        dma((2,)), dma((2,)),
        dma((n_tp,)), dma((n_tp,)),
        dma((n_tp,)), dma((n_tp,)),
        dma((n_sp,)), dma((n_sp,)),
        dma((n_sp, n_tp)),
        dma((n_z, n_tp)), dma((n_z,)), dma((n_z, n_tp)),
        dma((n_tp, CHUNKS)), dma((n_tp, CHUNKS)),
        dma((n_z,)), dma((n_z,)),
        dma((n_z, n_tp)), dma((n_z, n_tp)),
        dma((n_z,)), dma((n_z,)),
    ]
    return pl.pallas_call(
        functools.partial(kernel, n_sp, n_tp),
        out_shape=jax.ShapeDtypeStruct((feats, pos), BF16),
        in_specs=[vmem] * 7 + [anywhere] + [vmem] * 3 + [anywhere] * 6,
        out_specs=vmem,
        scratch_shapes=scratch,
        compiler_params=pltpu.CompilerParams(
            collective_id=0, has_side_effects=True, vmem_limit_bytes=64 * 1024 * 1024 - 65536
        ),
    )(
        stream, values_in, in_gate, out_gate, documents.reshape(1, pos), conv_taps,
        head_gain.reshape(1, chans), mix_weight, norm_gain.reshape(1, feats), routes,
        route_weight, expert_gate, expert_up, expert_down, shared_gate, shared_up, shared_down,
    )


def solution(mesh):
    in_specs = (
        P("tp", "sp"),
        P("tp", "sp"),
        P("tp", "sp"),
        P("tp", "sp"),
        P("sp"),
        P(None, "tp"),
        P("tp"),
        P("tp", None),
        P("tp"),
        P("sp", None),
        P("sp", None),
        P("sp", None, "tp"),
        P("sp", None, "tp"),
        P("sp", None, "tp"),
        P(None, "tp"),
        P(None, "tp"),
        P("tp", None),
    )
    body = functools.partial(local, mesh.shape["sp"], mesh.shape["tp"])
    return jax.shard_map(
        body, mesh=mesh, in_specs=in_specs, out_specs=P("tp", "sp"), check_vma=False
    )
```

```python
import functools

import jax
import jax.numpy as jnp
from jax import lax
from jax.experimental import pallas as pl
from jax.experimental.pallas import tpu as pltpu
from jax.sharding import PartitionSpec as P

HEAD = 64
CORES = 2
CHUNKS = 8
SUB = 8
epsilon = 1e-06
MESH = pl.DeviceIdType.MESH
F32 = jnp.float32
BF16 = jnp.bfloat16


def flipped(index, mask):
    bit = 1
    out = index
    while bit <= mask:
        if mask & bit:
            out = out + bit - 2 * bit * lax.rem(lax.div(index, bit), 2)
        bit *= 2
    return out


def dot(left, right):
    return jnp.dot(left, right, preferred_element_type=F32)


def silu(value):
    return value / (1.0 + jnp.exp(-value))


def column_of(row, width):
    return jnp.broadcast_to(row, (width, row.shape[1])).T


def kernel(
    n_sp, n_tp,
    stream, values_in, in_gate, out_gate, documents, conv_taps, head_gain, mix_weight,
    norm_gain, routes, route_weight, expert_gate, expert_up, expert_down,
    shared_gate, shared_up, shared_down,
    out,
    mix_w, gate_w, up_w, sgate_w, sup_w, sdown_w, down_w,
    tail_s, prev_r, prev_docs, mix_s, mix_r, hidden_v, x_all, ss_s, ss_r, meta_r,
    mid_v, shared_v, acc_v, pr_s, pr_r, rs_s, rs_r, rd_r, zr_s, zr_r,
    load_sem, local_sem, halo_send, halo_recv, mix_send, mix_recv, ss_send, ss_recv,
    meta_send, meta_recv, x_recv, xs_tp, xs_z, xs_d, xs_p, wd_send, wd_recv,
    pr_send, pr_recv, rs_send, rs_recv, zr_send, zr_recv,
):
    sp = lax.axis_index("sp")
    tp = lax.axis_index("tp")
    z = lax.div(sp, CORES)
    core = lax.rem(sp, CORES)
    n_z = n_sp // CORES
    feats, pos = stream.shape
    chans = values_in.shape[0]
    width = feats * n_tp
    hid = gate_w.shape[1]
    partner = {"sp": z * CORES + 1 - core}
    peers = [flipped(tp, d) for d in range(1, n_tp)]
    square = n_tp == 4
    near = peers[:2] if square else peers
    layers = [flipped(z, d) for d in range(n_z)]
    pending = []

    def send(src, dst, ssem, rsem, device):
        copy = pltpu.make_async_remote_copy(
            src_ref=src, dst_ref=dst, send_sem=ssem, recv_sem=rsem,
            device_id=device, device_id_type=MESH,
        )
        copy.start()
        pending.append(copy)

    def arrived(dst, rsem):
        pltpu.make_async_remote_copy(
            src_ref=dst, dst_ref=dst, send_sem=rsem, recv_sem=rsem,
            device_id=partner, device_id_type=MESH,
        ).wait_recv()

    loads = [
        pltpu.make_async_copy(src, dst, load_sem.at[i])
        for i, (src, dst) in enumerate([
            (mix_weight, mix_w), (shared_gate, sgate_w), (shared_up, sup_w),
            (shared_down, sdown_w), (expert_gate.at[0], gate_w), (expert_up.at[0], up_w),
        ])
    ]
    loads[0].start()

    barrier = pltpu.get_barrier_semaphore()
    for peer in peers:
        pl.semaphore_signal(barrier, inc=1, device_id={"tp": peer}, device_id_type=MESH)
    for d in range(1, n_sp):
        pl.semaphore_signal(
            barrier, inc=1, device_id={"sp": lax.rem(sp + d, n_sp)}, device_id_type=MESH
        )
    pl.semaphore_wait(barrier, n_tp - 1 + n_sp - 1)

    product = values_in[...].astype(F32) * in_gate[...].astype(F32)
    tail_s[...] = product.T[pos - SUB:, :]
    after = {"sp": lax.rem(sp + 1, n_sp)}
    send(tail_s, prev_r.at[pl.ds(pos - SUB, SUB)], halo_send.at[0], halo_recv.at[0], after)
    send(documents, prev_docs, halo_send.at[1], halo_recv.at[1], after)

    rows = hid // CHUNKS

    def send_down(chunk):
        for d, peer in enumerate(peers):
            start = pl.multiple_of(peer * hid + chunk * rows, rows)
            send(
                expert_down.at[0, pl.ds(start, rows), :],
                down_w.at[tp, pl.ds(chunk * rows, rows), :],
                wd_send.at[d, chunk], wd_recv.at[tp, chunk], {"tp": peer},
            )

    for chunk in (0, 1):
        send_down(chunk)
    own_down = pltpu.make_async_copy(
        expert_down.at[0, pl.ds(pl.multiple_of(tp * hid, hid), hid), :], down_w.at[tp], local_sem
    )
    for load in loads[1:]:
        load.start()
    own_down.start()

    named = routes[...]
    weights = route_weight[...]
    meta_rows = meta_r.shape[1]
    lane = lax.broadcasted_iota(jnp.int32, (pos, pos), 1)
    table = jnp.zeros((pos, pos), F32)
    for k in range(routes.shape[1]):
        table = table + jnp.where(lane == named[:, k:k + 1], weights[:, k:k + 1], 0.0)
    table = table.T[:meta_rows]
    taps = [column_of(conv_taps[j:j + 1, :], pos) for j in range(3)]
    stream_t = stream[...].astype(F32).T

    prev_r[: pos - SUB, :] = jnp.zeros((pos - SUB, chans), F32)
    arrived(prev_r.at[pl.ds(pos - SUB, SUB)], halo_recv.at[0])
    arrived(prev_docs, halo_recv.at[1])
    before = prev_r[...].T
    docs = documents[...]
    docs_before = jnp.where(sp > 0, prev_docs[...], -1)
    lane_c = lax.broadcasted_iota(jnp.int32, (chans, pos), 1)
    lane_1 = lax.broadcasted_iota(jnp.int32, (1, pos), 1)
    convolved = taps[2] * product
    for shift in (1, 2):
        moved = jnp.where(lane_c < shift, pltpu.roll(before, shift, 1), pltpu.roll(product, shift, 1))
        ids = jnp.where(lane_1 < shift, pltpu.roll(docs_before, shift, 1), pltpu.roll(docs, shift, 1))
        convolved = convolved + jnp.where(ids == docs, taps[2 - shift] * moved, 0.0)
    mixed = out_gate[...].astype(F32) * convolved
    heads = mixed.reshape(chans // HEAD, HEAD, pos)
    heads = heads * lax.rsqrt(jnp.mean(heads * heads, axis=1, keepdims=True) + epsilon)
    heads_t = (heads.reshape(chans, pos).T * head_gain[...]).astype(BF16)

    loads[0].wait()
    for b, peer in enumerate(peers + [tp]):
        cols = pl.ds(pl.multiple_of(peer * feats, feats), feats)
        mix_s[b] = dot(heads_t, mix_w[:, cols]).astype(BF16)
        if b < n_tp - 1:
            send(mix_s.at[b], mix_r.at[b], mix_send.at[b], mix_recv.at[b], {"tp": peer})
    send_down(2)

    hidden = stream_t + mix_s[n_tp - 1].astype(F32)
    for b in range(n_tp - 1):
        arrived(mix_r.at[b], mix_recv.at[b])
        hidden = hidden + mix_r[b].astype(F32)
    hidden_v[...] = hidden
    x_all[sp, tp] = (hidden * norm_gain[...]).astype(BF16)
    own = x_all.at[sp, tp]
    for d in range(1, n_z):
        send(own, own, xs_z.at[d], x_recv.at[sp, tp], {"sp": layers[d] * CORES + core})
    for b, peer in enumerate(peers):
        send(own, own, xs_tp.at[0, b], x_recv.at[sp, tp], {"tp": peer})
    send(own, own, xs_p.at[0, 0], x_recv.at[sp, tp], partner)

    squares = jnp.sum(hidden * hidden, axis=1, keepdims=True)
    row = jnp.broadcast_to(squares, (pos, pos)).T[:SUB]
    ss_s[...] = row
    for b, peer in enumerate(peers):
        send(ss_s, ss_r.at[b], ss_send.at[b], ss_recv.at[b], {"tp": peer})
    send_down(3)
    for b in range(n_tp - 1):
        arrived(ss_r.at[b], ss_recv.at[b])
        row = row + ss_r[b]
    scale = lax.rsqrt(row[:1] / width + epsilon)
    at_row = lax.broadcasted_iota(jnp.int32, (meta_rows, pos), 0)
    meta_r[sp] = jnp.where(at_row == meta_rows - 1, scale, table)
    for d in range(1, n_sp):
        send(meta_r.at[sp], meta_r.at[sp], meta_send.at[d], meta_recv.at[sp],
             {"sp": lax.rem(sp + d, n_sp)})

    def to_partner(slot, b, group):
        block = x_all.at[group, peers[b]]
        arrived(block, x_recv.at[group, peers[b]])
        send(block, block, xs_p.at[slot, b + 1], x_recv.at[group, peers[b]], partner)

    def from_layer(d):
        group = layers[d] * CORES + core
        block = x_all.at[group, tp]
        arrived(block, x_recv.at[group, tp])
        for b, peer in enumerate(near):
            send(block, block, xs_tp.at[d, b], x_recv.at[group, tp], {"tp": peer})
        send(block, block, xs_p.at[d, 0], x_recv.at[group, tp], partner)

    for b in range(n_tp - 1):
        to_partner(0, b, sp)
    if square:
        block = x_all.at[sp, peers[2]]
        for d in range(1, n_z):
            send(block, block, xs_d.at[d], x_recv.at[sp, peers[2]],
                 {"sp": layers[d] * CORES + core})
    from_layer(1)
    for chunk in (4, 5):
        send_down(chunk)

    loads[1].wait()
    loads[2].wait()
    scale_own = column_of(scale, pos)[:, :1]
    gate = jnp.zeros((pos, hid), F32)
    upward = jnp.zeros((pos, hid), F32)
    for b in range(n_tp):
        block = x_all[sp, b]
        gate = gate + dot(block, sgate_w[b * feats:(b + 1) * feats, :])
        upward = upward + dot(block, sup_w[b * feats:(b + 1) * feats, :])
    shared_mid = (silu(gate * scale_own) * (upward * scale_own)).astype(BF16)
    loads[3].wait()
    shared_v[...] = dot(shared_mid, sdown_w[...])

    for d in range(2, n_z):
        from_layer(d)
    for chunk in (6, 7):
        send_down(chunk)

    loads[4].wait()
    loads[5].wait()
    for d in range(n_z):
        layer = layers[d]
        mine = layer * CORES + core
        other = layer * CORES + 1 - core
        if d > 0:
            for b in range(n_tp - 1):
                to_partner(d, b, mine)
            arrived(meta_r.at[mine], meta_recv.at[mine])
        arrived(meta_r.at[other], meta_recv.at[other])
        for b in range(n_tp):
            arrived(x_all.at[other, b], x_recv.at[other, b])
        gate = jnp.zeros((CORES * pos, hid), F32)
        upward = jnp.zeros((CORES * pos, hid), F32)
        for b in range(n_tp):
            block = x_all[pl.ds(layer * CORES, CORES), b].reshape(CORES * pos, feats)
            gate = gate + dot(block, gate_w[b * feats:(b + 1) * feats, :])
            upward = upward + dot(block, up_w[b * feats:(b + 1) * feats, :])
        scales = jnp.concatenate([
            column_of(meta_r[layer * CORES + i, meta_rows - 1:, :], pos)[:, :1]
            for i in range(CORES)
        ], axis=0)
        mid_v[layer] = (silu(gate * scales) * (upward * scales)).astype(BF16)

    own_down.wait()
    for peer in peers:
        for chunk in range(CHUNKS):
            arrived(down_w.at[peer, pl.ds(chunk * rows, rows), :], wd_recv.at[peer, chunk])

    order = list(range(2, n_z)) + [1, 0]
    half = pos // 2
    totals = {}

    def multiply(step):
        layer = layers[order[step]]
        weight = jnp.concatenate([
            column_of(meta_r[layer * CORES + i, pl.ds(sp, 1), :], pos)[:, :1]
            for i in range(CORES)
        ], axis=0)
        middle = mid_v[layer]
        for b in range(n_tp):
            term = dot(middle, down_w[b]) * weight
            lower, upper = term[:pos], term[pos:]
            pr_s[step, b] = jnp.where(core == 0, upper, lower).astype(BF16)
            acc_v[step % 3, b] = jnp.where(core == 0, lower, upper)
        send(pr_s.at[step], pr_r.at[step], pr_send.at[step], pr_recv.at[step], partner)

    def block_of(step, peer):
        term = acc_v[step % 3, peer] + pr_r[step, peer].astype(F32)
        if order[step] == 0:
            cols = pl.ds(pl.multiple_of(peer * feats, feats), feats)
            term = term + shared_v[:, cols]
        return term

    def cross(step):
        arrived(pr_r.at[step], pr_recv.at[step])
        if square:
            rs_s[step, 2] = block_of(step, peers[2]).astype(BF16)
            for b in range(2):
                part = pl.ds(b * half, half)
                send(rs_s.at[step, 2, part], rd_r.at[step, part], rs_send.at[step, 2 + b],
                     rs_recv.at[step, 2 + b], {"tp": peers[b]})
        rs_s[step, n_tp - 1] = block_of(step, tp).astype(BF16)

    def spread(step):
        if square:
            for b in range(2):
                part = pl.ds(b * half, half)
                arrived(rd_r.at[step, part], rs_recv.at[step, 2 + b])
        for b, peer in enumerate(near):
            term = block_of(step, peer)
            if square:
                part = slice((1 - b) * half, (2 - b) * half)
                extra = rd_r[step, part, :].astype(F32)
                fixed = term[b * half:(b + 1) * half]
                joined = [fixed, term[part] + extra]
                term = jnp.concatenate(joined if b == 0 else joined[::-1], axis=0)
            rs_s[step, b] = term.astype(BF16)
            send(rs_s.at[step, b], rs_r.at[step, b], rs_send.at[step, b],
                 rs_recv.at[step, b], {"tp": peer})

    def gathered(step):
        total = rs_s[step, n_tp - 1].astype(F32)
        for b in range(len(near)):
            arrived(rs_r.at[step, b], rs_recv.at[step, b])
            total = total + rs_r[step, b].astype(F32)
        d = order[step]
        if d == 0:
            totals[0] = total
        else:
            zr_s[d] = total.astype(BF16)
            send(zr_s.at[d], zr_r.at[d], zr_send.at[d], zr_recv.at[d],
                 {"sp": layers[d] * CORES + core})

    for step in range(n_z + 3):
        for lag, stage in enumerate((multiply, cross, spread, gathered)):
            if 0 <= step - lag < n_z:
                stage(step - lag)

    result = hidden_v[...] + totals[0]
    for d in range(1, n_z):
        arrived(zr_r.at[d], zr_recv.at[d])
        result = result + zr_r[d].astype(F32)
    out[...] = result.T.astype(BF16)
    for copy in pending:
        copy.wait_send()


def local(n_sp, n_tp, *args):
    (stream, values_in, in_gate, out_gate, documents, conv_taps, head_gain, mix_weight,
     norm_gain, routes, route_weight, expert_gate, expert_up, expert_down,
     shared_gate, shared_up, shared_down) = args
    feats, pos = stream.shape
    chans = values_in.shape[0]
    width = feats * n_tp
    hid = expert_gate.shape[2]
    n_z = n_sp // CORES
    meta_rows = -(-(n_sp + 1) // SUB) * SUB
    vmem = pl.BlockSpec(memory_space=pltpu.VMEM)
    anywhere = pl.BlockSpec(memory_space=pl.ANY)
    dma = pltpu.SemaphoreType.DMA
    scratch = [
        pltpu.VMEM((chans, width), BF16),
        pltpu.VMEM((width, hid), BF16),
        pltpu.VMEM((width, hid), BF16),
        pltpu.VMEM((width, hid), BF16),
        pltpu.VMEM((width, hid), BF16),
        pltpu.VMEM((hid, width), BF16),
        pltpu.VMEM((n_tp, hid, feats), BF16),
        pltpu.VMEM((SUB, chans), F32),
        pltpu.VMEM((pos, chans), F32),
        pltpu.VMEM((1, pos), jnp.int32),
        pltpu.VMEM((n_tp, pos, feats), BF16),
        pltpu.VMEM((n_tp, pos, feats), BF16),
        pltpu.VMEM((pos, feats), F32),
        pltpu.VMEM((n_sp, n_tp, pos, feats), BF16),
        pltpu.VMEM((SUB, pos), F32),
        pltpu.VMEM((n_tp, SUB, pos), F32),
        pltpu.VMEM((n_sp, meta_rows, pos), F32),
        pltpu.VMEM((n_z, CORES * pos, hid), BF16),
        pltpu.VMEM((pos, width), F32),
        pltpu.VMEM((3, n_tp, pos, feats), F32),
        pltpu.VMEM((n_z, n_tp, pos, feats), BF16),
        pltpu.VMEM((n_z, n_tp, pos, feats), BF16),
        pltpu.VMEM((n_z, n_tp, pos, feats), BF16),
        pltpu.VMEM((n_z, n_tp, pos, feats), BF16),
        pltpu.VMEM((n_z if n_tp == 4 else 1, pos, feats), BF16),
        pltpu.VMEM((n_z, pos, feats), BF16),
        pltpu.VMEM((n_z, pos, feats), BF16),
        dma((6,)), dma,
        dma((2,)), dma((2,)),
        dma((n_tp,)), dma((n_tp,)),
        dma((n_tp,)), dma((n_tp,)),
        dma((n_sp,)), dma((n_sp,)),
        dma((n_sp, n_tp)),
        dma((n_z, n_tp)), dma((n_z,)), dma((n_z,)), dma((n_z, n_tp)),
        dma((n_tp, CHUNKS)), dma((n_tp, CHUNKS)),
        dma((n_z,)), dma((n_z,)),
        dma((n_z, n_tp)), dma((n_z, n_tp)),
        dma((n_z,)), dma((n_z,)),
    ]
    return pl.pallas_call(
        functools.partial(kernel, n_sp, n_tp),
        out_shape=jax.ShapeDtypeStruct((feats, pos), BF16),
        in_specs=[vmem] * 7 + [anywhere] + [vmem] * 3 + [anywhere] * 6,
        out_specs=vmem,
        scratch_shapes=scratch,
        compiler_params=pltpu.CompilerParams(
            collective_id=0, has_side_effects=True, vmem_limit_bytes=64 * 1024 * 1024 - 65536
        ),
    )(
        stream, values_in, in_gate, out_gate, documents.reshape(1, pos), conv_taps,
        head_gain.reshape(1, chans), mix_weight, norm_gain.reshape(1, feats), routes,
        route_weight, expert_gate, expert_up, expert_down, shared_gate, shared_up, shared_down,
    )


def solution(mesh):
    in_specs = (
        P("tp", "sp"),
        P("tp", "sp"),
        P("tp", "sp"),
        P("tp", "sp"),
        P("sp"),
        P(None, "tp"),
        P("tp"),
        P("tp", None),
        P("tp"),
        P("sp", None),
        P("sp", None),
        P("sp", None, "tp"),
        P("sp", None, "tp"),
        P("sp", None, "tp"),
        P(None, "tp"),
        P(None, "tp"),
        P("tp", None),
    )
    body = functools.partial(local, mesh.shape["sp"], mesh.shape["tp"])
    return jax.shard_map(
        body, mesh=mesh, in_specs=in_specs, out_specs=P("tp", "sp"), check_vma=False
    )
```

```python
import functools

import jax
import jax.numpy as jnp
from jax import lax
from jax.experimental import pallas as pl
from jax.experimental.pallas import tpu as pltpu
from jax.sharding import PartitionSpec as P

HEAD = 64
CORES = 2
CHUNKS = 8
SUB = 8
epsilon = 1e-06
MESH = pl.DeviceIdType.MESH
F32 = jnp.float32
BF16 = jnp.bfloat16


def flipped(index, mask):
    bit = 1
    out = index
    while bit <= mask:
        if mask & bit:
            out = out + bit - 2 * bit * lax.rem(lax.div(index, bit), 2)
        bit *= 2
    return out


def dot(left, right):
    return jnp.dot(left, right, preferred_element_type=F32)


def silu(value):
    return value / (1.0 + jnp.exp(-value))


def column_of(row, width):
    return jnp.broadcast_to(row, (width, row.shape[1])).T


def kernel(
    n_sp, n_tp,
    stream, values_in, in_gate, out_gate, documents, conv_taps, head_gain, mix_weight,
    norm_gain, routes, route_weight, expert_gate, expert_up, expert_down,
    shared_gate, shared_up, shared_down,
    out,
    mix_w, gate_w, up_w, sgate_w, sup_w, sdown_w, down_w,
    tail_s, prev_r, prev_docs, mix_s, mix_r, hidden_v, x_all, ss_s, ss_r, meta_r,
    mid_v, shared_v, acc_v, pr_s, pr_r, rs_s, rs_r, rd_r, zr_s, zr_r,
    load_sem, local_sem, halo_send, halo_recv, mix_send, mix_recv, ss_send, ss_recv,
    meta_send, meta_recv, x_recv, xs_tp, xs_z, xs_d, xs_p, wd_send, wd_recv,
    pr_send, pr_recv, rs_send, rs_recv, zr_send, zr_recv,
):
    sp = lax.axis_index("sp")
    tp = lax.axis_index("tp")
    z = lax.div(sp, CORES)
    core = lax.rem(sp, CORES)
    n_z = n_sp // CORES
    feats, pos = stream.shape
    chans = values_in.shape[0]
    width = feats * n_tp
    hid = gate_w.shape[1]
    partner = {"sp": z * CORES + 1 - core}
    peers = [flipped(tp, d) for d in range(1, n_tp)]
    square = n_tp == 4
    near = peers[:2] if square else peers
    layers = [flipped(z, d) for d in range(n_z)]
    pending = []

    def send(src, dst, ssem, rsem, device):
        copy = pltpu.make_async_remote_copy(
            src_ref=src, dst_ref=dst, send_sem=ssem, recv_sem=rsem,
            device_id=device, device_id_type=MESH,
        )
        copy.start()
        pending.append(copy)

    def arrived(dst, rsem):
        pltpu.make_async_remote_copy(
            src_ref=dst, dst_ref=dst, send_sem=rsem, recv_sem=rsem,
            device_id=partner, device_id_type=MESH,
        ).wait_recv()

    loads = [
        pltpu.make_async_copy(src, dst, load_sem.at[i])
        for i, (src, dst) in enumerate([
            (mix_weight, mix_w), (shared_gate, sgate_w), (shared_up, sup_w),
            (shared_down, sdown_w), (expert_gate.at[0], gate_w), (expert_up.at[0], up_w),
        ])
    ]
    loads[0].start()

    barrier = pltpu.get_barrier_semaphore()
    for peer in peers:
        pl.semaphore_signal(barrier, inc=1, device_id={"tp": peer}, device_id_type=MESH)
    for d in range(1, n_sp):
        pl.semaphore_signal(
            barrier, inc=1, device_id={"sp": lax.rem(sp + d, n_sp)}, device_id_type=MESH
        )
    pl.semaphore_wait(barrier, n_tp - 1 + n_sp - 1)

    product = values_in[...].astype(F32) * in_gate[...].astype(F32)
    tail_s[...] = product.T[pos - SUB:, :]
    after = {"sp": lax.rem(sp + 1, n_sp)}
    send(tail_s, prev_r.at[pl.ds(pos - SUB, SUB)], halo_send.at[0], halo_recv.at[0], after)
    send(documents, prev_docs, halo_send.at[1], halo_recv.at[1], after)

    rows = hid // CHUNKS

    def send_down(chunk):
        for d, peer in enumerate(peers):
            start = pl.multiple_of(peer * hid + chunk * rows, rows)
            send(
                expert_down.at[0, pl.ds(start, rows), :],
                down_w.at[tp, pl.ds(chunk * rows, rows), :],
                wd_send.at[d, chunk], wd_recv.at[tp, chunk], {"tp": peer},
            )

    for chunk in (0, 1):
        send_down(chunk)
    own_down = pltpu.make_async_copy(
        expert_down.at[0, pl.ds(pl.multiple_of(tp * hid, hid), hid), :], down_w.at[tp], local_sem
    )
    for load in loads[1:]:
        load.start()
    own_down.start()

    named = routes[...]
    weights = route_weight[...]
    meta_rows = meta_r.shape[1]
    at_row = lax.broadcasted_iota(jnp.int32, (meta_rows, pos), 0)
    table = jnp.zeros((meta_rows, pos), F32)
    for k in range(routes.shape[0]):
        table = table + jnp.where(at_row == named[k:k + 1, :], weights[k:k + 1, :], 0.0)
    taps = [column_of(conv_taps[j:j + 1, :], pos) for j in range(3)]
    stream_t = stream[...].astype(F32).T

    prev_r[: pos - SUB, :] = jnp.zeros((pos - SUB, chans), F32)
    arrived(prev_r.at[pl.ds(pos - SUB, SUB)], halo_recv.at[0])
    arrived(prev_docs, halo_recv.at[1])
    before = prev_r[...].T
    docs = documents[...]
    docs_before = jnp.where(sp > 0, prev_docs[...], -1)
    lane_c = lax.broadcasted_iota(jnp.int32, (chans, pos), 1)
    lane_1 = lax.broadcasted_iota(jnp.int32, (1, pos), 1)
    convolved = taps[2] * product
    for shift in (1, 2):
        moved = jnp.where(lane_c < shift, pltpu.roll(before, shift, 1), pltpu.roll(product, shift, 1))
        ids = jnp.where(lane_1 < shift, pltpu.roll(docs_before, shift, 1), pltpu.roll(docs, shift, 1))
        convolved = convolved + jnp.where(ids == docs, taps[2 - shift] * moved, 0.0)
    mixed = out_gate[...].astype(F32) * convolved
    heads = mixed.reshape(chans // HEAD, HEAD, pos)
    heads = heads * lax.rsqrt(jnp.mean(heads * heads, axis=1, keepdims=True) + epsilon)
    heads_t = (heads.reshape(chans, pos).T * head_gain[...]).astype(BF16)

    loads[0].wait()
    for b, peer in enumerate(peers + [tp]):
        cols = pl.ds(pl.multiple_of(peer * feats, feats), feats)
        mix_s[b] = dot(heads_t, mix_w[:, cols]).astype(BF16)
        if b < n_tp - 1:
            send(mix_s.at[b], mix_r.at[b], mix_send.at[b], mix_recv.at[b], {"tp": peer})
    send_down(2)

    hidden = stream_t + mix_s[n_tp - 1].astype(F32)
    for b in range(n_tp - 1):
        arrived(mix_r.at[b], mix_recv.at[b])
        hidden = hidden + mix_r[b].astype(F32)
    hidden_v[...] = hidden
    x_all[sp, tp] = (hidden * norm_gain[...]).astype(BF16)
    own = x_all.at[sp, tp]
    for d in range(1, n_z):
        send(own, own, xs_z.at[d], x_recv.at[sp, tp], {"sp": layers[d] * CORES + core})
    for b, peer in enumerate(peers):
        send(own, own, xs_tp.at[0, b], x_recv.at[sp, tp], {"tp": peer})
    send(own, own, xs_p.at[0, 0], x_recv.at[sp, tp], partner)

    squares = jnp.sum(hidden * hidden, axis=1, keepdims=True)
    row = jnp.broadcast_to(squares, (pos, pos)).T[:SUB]
    ss_s[...] = row
    for b, peer in enumerate(peers):
        send(ss_s, ss_r.at[b], ss_send.at[b], ss_recv.at[b], {"tp": peer})
    send_down(3)
    for b in range(n_tp - 1):
        arrived(ss_r.at[b], ss_recv.at[b])
        row = row + ss_r[b]
    scale = lax.rsqrt(row[:1] / width + epsilon)
    meta_r[sp] = jnp.where(at_row == meta_rows - 1, scale, table)
    for d in range(1, n_sp):
        send(meta_r.at[sp], meta_r.at[sp], meta_send.at[d], meta_recv.at[sp],
             {"sp": lax.rem(sp + d, n_sp)})

    def to_partner(slot, b, group):
        block = x_all.at[group, peers[b]]
        arrived(block, x_recv.at[group, peers[b]])
        send(block, block, xs_p.at[slot, b + 1], x_recv.at[group, peers[b]], partner)

    def from_layer(d):
        group = layers[d] * CORES + core
        block = x_all.at[group, tp]
        arrived(block, x_recv.at[group, tp])
        for b, peer in enumerate(near):
            send(block, block, xs_tp.at[d, b], x_recv.at[group, tp], {"tp": peer})
        send(block, block, xs_p.at[d, 0], x_recv.at[group, tp], partner)

    for b in range(n_tp - 1):
        to_partner(0, b, sp)
    if square:
        block = x_all.at[sp, peers[2]]
        for d in range(1, n_z):
            send(block, block, xs_d.at[d], x_recv.at[sp, peers[2]],
                 {"sp": layers[d] * CORES + core})
    from_layer(1)
    for chunk in range(4, CHUNKS):
        send_down(chunk)

    loads[1].wait()
    loads[2].wait()
    scale_own = column_of(scale, pos)[:, :1]
    gate = jnp.zeros((pos, hid), F32)
    upward = jnp.zeros((pos, hid), F32)
    for b in range(n_tp):
        block = x_all[sp, b]
        gate = gate + dot(block, sgate_w[b * feats:(b + 1) * feats, :])
        upward = upward + dot(block, sup_w[b * feats:(b + 1) * feats, :])
    shared_mid = (silu(gate * scale_own) * (upward * scale_own)).astype(BF16)
    loads[3].wait()
    shared_v[...] = dot(shared_mid, sdown_w[...])

    for d in range(2, n_z):
        from_layer(d)

    loads[4].wait()
    loads[5].wait()
    def widen(d):
        layer = layers[d]
        mine = layer * CORES + core
        other = layer * CORES + 1 - core
        if d > 0:
            for b in range(n_tp - 1):
                to_partner(d, b, mine)
            arrived(meta_r.at[mine], meta_recv.at[mine])
        arrived(meta_r.at[other], meta_recv.at[other])
        for b in range(n_tp):
            arrived(x_all.at[other, b], x_recv.at[other, b])
        gate = jnp.zeros((CORES * pos, hid), F32)
        upward = jnp.zeros((CORES * pos, hid), F32)
        for b in range(n_tp):
            block = x_all[pl.ds(layer * CORES, CORES), b].reshape(CORES * pos, feats)
            gate = gate + dot(block, gate_w[b * feats:(b + 1) * feats, :])
            upward = upward + dot(block, up_w[b * feats:(b + 1) * feats, :])
        scales = jnp.concatenate([
            column_of(meta_r[layer * CORES + i, meta_rows - 1:, :], pos)[:, :1]
            for i in range(CORES)
        ], axis=0)
        mid_v[layer] = (silu(gate * scales) * (upward * scales)).astype(BF16)

    widen(0)
    if n_z > 1:
        widen(1)
    own_down.wait()
    for peer in peers:
        for chunk in range(CHUNKS):
            arrived(down_w.at[peer, pl.ds(chunk * rows, rows), :], wd_recv.at[peer, chunk])

    order = list(range(1, n_z)) + [0]
    half = pos // 2
    totals = {}

    def multiply(step):
        layer = layers[order[step]]
        weight = jnp.concatenate([
            column_of(meta_r[layer * CORES + i, pl.ds(sp, 1), :], pos)[:, :1]
            for i in range(CORES)
        ], axis=0)
        middle = mid_v[layer]
        for b in range(n_tp):
            term = dot(middle, down_w[b]) * weight
            lower, upper = term[:pos], term[pos:]
            pr_s[step, b] = jnp.where(core == 0, upper, lower).astype(BF16)
            acc_v[step % 3, b] = jnp.where(core == 0, lower, upper)
        send(pr_s.at[step], pr_r.at[step], pr_send.at[step], pr_recv.at[step], partner)

    def block_of(step, peer):
        term = acc_v[step % 3, peer] + pr_r[step, peer].astype(F32)
        if order[step] == 0:
            cols = pl.ds(pl.multiple_of(peer * feats, feats), feats)
            term = term + shared_v[:, cols]
        return term

    def cross(step):
        arrived(pr_r.at[step], pr_recv.at[step])
        if square:
            rs_s[step, 2] = block_of(step, peers[2]).astype(BF16)
            for b in range(2):
                part = pl.ds(b * half, half)
                send(rs_s.at[step, 2, part], rd_r.at[step, part], rs_send.at[step, 2 + b],
                     rs_recv.at[step, 2 + b], {"tp": peers[b]})
        rs_s[step, n_tp - 1] = block_of(step, tp).astype(BF16)

    def spread(step):
        if square:
            for b in range(2):
                part = pl.ds(b * half, half)
                arrived(rd_r.at[step, part], rs_recv.at[step, 2 + b])
        for b, peer in enumerate(near):
            term = block_of(step, peer)
            if square:
                part = slice((1 - b) * half, (2 - b) * half)
                extra = rd_r[step, part, :].astype(F32)
                fixed = term[b * half:(b + 1) * half]
                joined = [fixed, term[part] + extra]
                term = jnp.concatenate(joined if b == 0 else joined[::-1], axis=0)
            rs_s[step, b] = term.astype(BF16)
            send(rs_s.at[step, b], rs_r.at[step, b], rs_send.at[step, b],
                 rs_recv.at[step, b], {"tp": peer})

    def gathered(step):
        total = rs_s[step, n_tp - 1].astype(F32)
        for b in range(len(near)):
            arrived(rs_r.at[step, b], rs_recv.at[step, b])
            total = total + rs_r[step, b].astype(F32)
        d = order[step]
        if d == 0:
            totals[0] = total
        else:
            zr_s[d] = total.astype(BF16)
            send(zr_s.at[d], zr_r.at[d], zr_send.at[d], zr_recv.at[d],
                 {"sp": layers[d] * CORES + core})

    for step in range(n_z + 2):
        if step < n_z:
            multiply(step)
            if step + 2 < n_z:
                widen(step + 2)
        for lag, stage in enumerate((cross, spread, gathered)):
            if 0 <= step - lag < n_z:
                stage(step - lag)

    result = hidden_v[...] + totals[0]
    for d in range(1, n_z):
        arrived(zr_r.at[d], zr_recv.at[d])
        result = result + zr_r[d].astype(F32)
    out[...] = result.T.astype(BF16)
    for copy in pending:
        copy.wait_send()


def local(n_sp, n_tp, *args):
    (stream, values_in, in_gate, out_gate, documents, conv_taps, head_gain, mix_weight,
     norm_gain, routes, route_weight, expert_gate, expert_up, expert_down,
     shared_gate, shared_up, shared_down) = args
    feats, pos = stream.shape
    chans = values_in.shape[0]
    width = feats * n_tp
    hid = expert_gate.shape[2]
    n_z = n_sp // CORES
    meta_rows = -(-(n_sp + 1) // SUB) * SUB
    vmem = pl.BlockSpec(memory_space=pltpu.VMEM)
    anywhere = pl.BlockSpec(memory_space=pl.ANY)
    dma = pltpu.SemaphoreType.DMA
    scratch = [
        pltpu.VMEM((chans, width), BF16),
        pltpu.VMEM((width, hid), BF16),
        pltpu.VMEM((width, hid), BF16),
        pltpu.VMEM((width, hid), BF16),
        pltpu.VMEM((width, hid), BF16),
        pltpu.VMEM((hid, width), BF16),
        pltpu.VMEM((n_tp, hid, feats), BF16),
        pltpu.VMEM((SUB, chans), F32),
        pltpu.VMEM((pos, chans), F32),
        pltpu.VMEM((1, pos), jnp.int32),
        pltpu.VMEM((n_tp, pos, feats), BF16),
        pltpu.VMEM((n_tp, pos, feats), BF16),
        pltpu.VMEM((pos, feats), F32),
        pltpu.VMEM((n_sp, n_tp, pos, feats), BF16),
        pltpu.VMEM((SUB, pos), F32),
        pltpu.VMEM((n_tp, SUB, pos), F32),
        pltpu.VMEM((n_sp, meta_rows, pos), F32),
        pltpu.VMEM((n_z, CORES * pos, hid), BF16),
        pltpu.VMEM((pos, width), F32),
        pltpu.VMEM((3, n_tp, pos, feats), F32),
        pltpu.VMEM((n_z, n_tp, pos, feats), BF16),
        pltpu.VMEM((n_z, n_tp, pos, feats), BF16),
        pltpu.VMEM((n_z, n_tp, pos, feats), BF16),
        pltpu.VMEM((n_z, n_tp, pos, feats), BF16),
        pltpu.VMEM((n_z if n_tp == 4 else 1, pos, feats), BF16),
        pltpu.VMEM((n_z, pos, feats), BF16),
        pltpu.VMEM((n_z, pos, feats), BF16),
        dma((6,)), dma,
        dma((2,)), dma((2,)),
        dma((n_tp,)), dma((n_tp,)),
        dma((n_tp,)), dma((n_tp,)),
        dma((n_sp,)), dma((n_sp,)),
        dma((n_sp, n_tp)),
        dma((n_z, n_tp)), dma((n_z,)), dma((n_z,)), dma((n_z, n_tp)),
        dma((n_tp, CHUNKS)), dma((n_tp, CHUNKS)),
        dma((n_z,)), dma((n_z,)),
        dma((n_z, n_tp)), dma((n_z, n_tp)),
        dma((n_z,)), dma((n_z,)),
    ]
    return pl.pallas_call(
        functools.partial(kernel, n_sp, n_tp),
        out_shape=jax.ShapeDtypeStruct((feats, pos), BF16),
        in_specs=[vmem] * 7 + [anywhere] + [vmem] * 3 + [anywhere] * 6,
        out_specs=vmem,
        scratch_shapes=scratch,
        compiler_params=pltpu.CompilerParams(
            collective_id=0, has_side_effects=True, vmem_limit_bytes=64 * 1024 * 1024 - 65536
        ),
    )(
        stream, values_in, in_gate, out_gate, documents.reshape(1, pos), conv_taps,
        head_gain.reshape(1, chans), mix_weight, norm_gain.reshape(1, feats), routes.T,
        route_weight.T, expert_gate, expert_up, expert_down, shared_gate, shared_up, shared_down,
    )


def solution(mesh):
    in_specs = (
        P("tp", "sp"),
        P("tp", "sp"),
        P("tp", "sp"),
        P("tp", "sp"),
        P("sp"),
        P(None, "tp"),
        P("tp"),
        P("tp", None),
        P("tp"),
        P("sp", None),
        P("sp", None),
        P("sp", None, "tp"),
        P("sp", None, "tp"),
        P("sp", None, "tp"),
        P(None, "tp"),
        P(None, "tp"),
        P("tp", None),
    )
    body = functools.partial(local, mesh.shape["sp"], mesh.shape["tp"])
    return jax.shard_map(
        body, mesh=mesh, in_specs=in_specs, out_specs=P("tp", "sp"), check_vma=False
    )
```

```python
import functools

import jax
import jax.numpy as jnp
from jax import lax
from jax.experimental import pallas as pl
from jax.experimental.pallas import tpu as pltpu
from jax.sharding import PartitionSpec as P

HEAD = 64
CORES = 2
CHUNKS = 8
SUB = 8
epsilon = 1e-06
MESH = pl.DeviceIdType.MESH
F32 = jnp.float32
BF16 = jnp.bfloat16


def flipped(index, mask):
    bit = 1
    out = index
    while bit <= mask:
        if mask & bit:
            out = out + bit - 2 * bit * lax.rem(lax.div(index, bit), 2)
        bit *= 2
    return out


def dot(left, right):
    return jnp.dot(left, right, preferred_element_type=F32)


def silu(value):
    return value / (1.0 + jnp.exp(-value))


def column_of(row, width):
    return jnp.broadcast_to(row, (width, row.shape[1])).T


def kernel(
    n_sp, n_tp,
    stream, values_in, in_gate, out_gate, documents, conv_taps, head_gain, mix_weight,
    norm_gain, routes, route_weight, expert_gate, expert_up, expert_down,
    shared_gate, shared_up, shared_down,
    out,
    mix_w, gate_w, up_w, sgate_w, sup_w, sdown_w, down_w,
    tail_s, prev_r, prev_docs, mix_s, mix_r, hidden_v, x_all, ss_s, ss_r, meta_r,
    mid_v, shared_v, acc_v, pr_s, pr_r, rs_s, rs_r, rd_r, rz_r, zr_s, zr_r,
    load_sem, local_sem, halo_send, halo_recv, mix_send, mix_recv, ss_send, ss_recv,
    meta_send, meta_recv, x_recv, xs_tp, xs_z, xs_d, xs_n, xs_p, wd_send, wd_recv,
    pr_send, pr_recv, rs_send, rs_recv, zr_send, zr_recv, rz_send, rz_recv,
):
    sp = lax.axis_index("sp")
    tp = lax.axis_index("tp")
    z = lax.div(sp, CORES)
    core = lax.rem(sp, CORES)
    n_z = n_sp // CORES
    feats, pos = stream.shape
    chans = values_in.shape[0]
    width = feats * n_tp
    hid = gate_w.shape[1]
    partner = {"sp": z * CORES + 1 - core}
    peers = [flipped(tp, d) for d in range(1, n_tp)]
    square = n_tp == 4 and n_z > 1
    near = peers[:2] if square else peers
    layers = [flipped(z, d) for d in range(n_z)]
    pending = []

    def send(src, dst, ssem, rsem, device):
        copy = pltpu.make_async_remote_copy(
            src_ref=src, dst_ref=dst, send_sem=ssem, recv_sem=rsem,
            device_id=device, device_id_type=MESH,
        )
        copy.start()
        pending.append(copy)

    def arrived(dst, rsem):
        pltpu.make_async_remote_copy(
            src_ref=dst, dst_ref=dst, send_sem=rsem, recv_sem=rsem,
            device_id=partner, device_id_type=MESH,
        ).wait_recv()

    loads = [
        pltpu.make_async_copy(src, dst, load_sem.at[i])
        for i, (src, dst) in enumerate([
            (mix_weight, mix_w), (shared_gate, sgate_w), (shared_up, sup_w),
            (shared_down, sdown_w), (expert_gate.at[0], gate_w), (expert_up.at[0], up_w),
        ])
    ]
    loads[0].start()

    barrier = pltpu.get_barrier_semaphore()
    for peer in peers:
        pl.semaphore_signal(barrier, inc=1, device_id={"tp": peer}, device_id_type=MESH)
    for d in range(1, n_sp):
        pl.semaphore_signal(
            barrier, inc=1, device_id={"sp": lax.rem(sp + d, n_sp)}, device_id_type=MESH
        )
    pl.semaphore_wait(barrier, n_tp - 1 + n_sp - 1)

    product = values_in[...].astype(F32) * in_gate[...].astype(F32)
    tail_s[...] = product.T[pos - SUB:, :]
    after = {"sp": lax.rem(sp + 1, n_sp)}
    send(tail_s, prev_r.at[pl.ds(pos - SUB, SUB)], halo_send.at[0], halo_recv.at[0], after)
    send(documents, prev_docs, halo_send.at[1], halo_recv.at[1], after)

    rows = hid // CHUNKS

    def send_down(chunk):
        for d, peer in enumerate(peers):
            start = pl.multiple_of(peer * hid + chunk * rows, rows)
            send(
                expert_down.at[0, pl.ds(start, rows), :],
                down_w.at[tp, pl.ds(chunk * rows, rows), :],
                wd_send.at[d, chunk], wd_recv.at[tp, chunk], {"tp": peer},
            )

    for chunk in (0, 1):
        send_down(chunk)
    own_down = pltpu.make_async_copy(
        expert_down.at[0, pl.ds(pl.multiple_of(tp * hid, hid), hid), :], down_w.at[tp], local_sem
    )
    for load in loads[1:]:
        load.start()
    own_down.start()

    named = routes[...]
    weights = route_weight[...]
    meta_rows = meta_r.shape[1]
    at_row = lax.broadcasted_iota(jnp.int32, (meta_rows, pos), 0)
    table = jnp.zeros((meta_rows, pos), F32)
    for k in range(routes.shape[0]):
        table = table + jnp.where(at_row == named[k:k + 1, :], weights[k:k + 1, :], 0.0)
    taps = [column_of(conv_taps[j:j + 1, :], pos) for j in range(3)]
    stream_t = stream[...].astype(F32).T

    prev_r[: pos - SUB, :] = jnp.zeros((pos - SUB, chans), F32)
    arrived(prev_r.at[pl.ds(pos - SUB, SUB)], halo_recv.at[0])
    arrived(prev_docs, halo_recv.at[1])
    before = prev_r[...].T
    docs = documents[...]
    docs_before = jnp.where(sp > 0, prev_docs[...], -1)
    lane_c = lax.broadcasted_iota(jnp.int32, (chans, pos), 1)
    lane_1 = lax.broadcasted_iota(jnp.int32, (1, pos), 1)
    convolved = taps[2] * product
    for shift in (1, 2):
        moved = jnp.where(lane_c < shift, pltpu.roll(before, shift, 1), pltpu.roll(product, shift, 1))
        ids = jnp.where(lane_1 < shift, pltpu.roll(docs_before, shift, 1), pltpu.roll(docs, shift, 1))
        convolved = convolved + jnp.where(ids == docs, taps[2 - shift] * moved, 0.0)
    mixed = out_gate[...].astype(F32) * convolved
    heads = mixed.reshape(chans // HEAD, HEAD, pos)
    heads = heads * lax.rsqrt(jnp.mean(heads * heads, axis=1, keepdims=True) + epsilon)
    heads_t = (heads.reshape(chans, pos).T * head_gain[...]).astype(BF16)

    loads[0].wait()
    for b, peer in enumerate(peers + [tp]):
        cols = pl.ds(pl.multiple_of(peer * feats, feats), feats)
        mix_s[b] = dot(heads_t, mix_w[:, cols]).astype(BF16)
        if b < n_tp - 1:
            send(mix_s.at[b], mix_r.at[b], mix_send.at[b], mix_recv.at[b], {"tp": peer})
    send_down(2)

    hidden = stream_t + mix_s[n_tp - 1].astype(F32)
    for b in range(n_tp - 1):
        arrived(mix_r.at[b], mix_recv.at[b])
        hidden = hidden + mix_r[b].astype(F32)
    hidden_v[...] = hidden
    x_all[sp, tp] = (hidden * norm_gain[...]).astype(BF16)
    own = x_all.at[sp, tp]
    for d in range(1, n_z):
        send(own, own, xs_z.at[d], x_recv.at[sp, tp], {"sp": layers[d] * CORES + core})
    for b, peer in enumerate(peers):
        send(own, own, xs_tp.at[0, b], x_recv.at[sp, tp], {"tp": peer})
    send(own, own, xs_p.at[0, 0], x_recv.at[sp, tp], partner)

    squares = jnp.sum(hidden * hidden, axis=1, keepdims=True)
    row = jnp.broadcast_to(squares, (pos, pos)).T[:SUB]
    ss_s[...] = row
    for b, peer in enumerate(peers):
        send(ss_s, ss_r.at[b], ss_send.at[b], ss_recv.at[b], {"tp": peer})
    send_down(3)
    for b in range(n_tp - 1):
        arrived(ss_r.at[b], ss_recv.at[b])
        row = row + ss_r[b]
    scale = lax.rsqrt(row[:1] / width + epsilon)
    meta_r[sp] = jnp.where(at_row == meta_rows - 1, scale, table)
    for d in range(1, n_sp):
        send(meta_r.at[sp], meta_r.at[sp], meta_send.at[d], meta_recv.at[sp],
             {"sp": lax.rem(sp + d, n_sp)})

    def to_partner(slot, b, group):
        block = x_all.at[group, peers[b]]
        arrived(block, x_recv.at[group, peers[b]])
        send(block, block, xs_p.at[slot, b + 1], x_recv.at[group, peers[b]], partner)

    def from_layer(d):
        group = layers[d] * CORES + core
        block = x_all.at[group, tp]
        arrived(block, x_recv.at[group, tp])
        for b, peer in enumerate([] if square and d == 1 else near):
            send(block, block, xs_tp.at[d, b], x_recv.at[group, tp], {"tp": peer})
        send(block, block, xs_p.at[d, 0], x_recv.at[group, tp], partner)

    for b in range(n_tp - 1):
        to_partner(0, b, sp)
        if square and b < 2:
            block = x_all.at[sp, peers[b]]
            send(block, block, xs_n.at[b], x_recv.at[sp, peers[b]],
                 {"sp": layers[1] * CORES + core})
    if square:
        block = x_all.at[sp, peers[2]]
        for d in range(1, n_z):
            send(block, block, xs_d.at[d], x_recv.at[sp, peers[2]],
                 {"sp": layers[d] * CORES + core})
    from_layer(1)
    for chunk in range(4, CHUNKS):
        send_down(chunk)

    loads[1].wait()
    loads[2].wait()
    scale_own = column_of(scale, pos)[:, :1]
    gate = jnp.zeros((pos, hid), F32)
    upward = jnp.zeros((pos, hid), F32)
    for b in range(n_tp):
        block = x_all[sp, b]
        gate = gate + dot(block, sgate_w[b * feats:(b + 1) * feats, :])
        upward = upward + dot(block, sup_w[b * feats:(b + 1) * feats, :])
    shared_mid = (silu(gate * scale_own) * (upward * scale_own)).astype(BF16)
    loads[3].wait()
    shared_v[...] = dot(shared_mid, sdown_w[...])

    for d in range(2, n_z):
        from_layer(d)

    loads[4].wait()
    loads[5].wait()
    def widen(d):
        layer = layers[d]
        mine = layer * CORES + core
        other = layer * CORES + 1 - core
        if d > 0:
            for b in range(n_tp - 1):
                to_partner(d, b, mine)
            arrived(meta_r.at[mine], meta_recv.at[mine])
        arrived(meta_r.at[other], meta_recv.at[other])
        for b in range(n_tp):
            arrived(x_all.at[other, b], x_recv.at[other, b])
        gate = jnp.zeros((CORES * pos, hid), F32)
        upward = jnp.zeros((CORES * pos, hid), F32)
        for b in range(n_tp):
            block = x_all[pl.ds(layer * CORES, CORES), b].reshape(CORES * pos, feats)
            gate = gate + dot(block, gate_w[b * feats:(b + 1) * feats, :])
            upward = upward + dot(block, up_w[b * feats:(b + 1) * feats, :])
        scales = jnp.concatenate([
            column_of(meta_r[layer * CORES + i, meta_rows - 1:, :], pos)[:, :1]
            for i in range(CORES)
        ], axis=0)
        mid_v[layer] = (silu(gate * scales) * (upward * scales)).astype(BF16)

    widen(0)
    if n_z > 1:
        widen(1)
    own_down.wait()
    for peer in peers:
        for chunk in range(CHUNKS):
            arrived(down_w.at[peer, pl.ds(chunk * rows, rows), :], wd_recv.at[peer, chunk])

    order = list(range(1, n_z)) + [0]
    half = pos // 2

    def direct(step):
        return square and order[step] == 1

    totals = {}

    def multiply(step):
        layer = layers[order[step]]
        weight = jnp.concatenate([
            column_of(meta_r[layer * CORES + i, pl.ds(sp, 1), :], pos)[:, :1]
            for i in range(CORES)
        ], axis=0)
        middle = mid_v[layer]
        for b in range(n_tp):
            term = dot(middle, down_w[b]) * weight
            lower, upper = term[:pos], term[pos:]
            pr_s[step, b] = jnp.where(core == 0, upper, lower).astype(BF16)
            acc_v[step % 3, b] = jnp.where(core == 0, lower, upper)
        send(pr_s.at[step], pr_r.at[step], pr_send.at[step], pr_recv.at[step], partner)

    def block_of(step, peer):
        term = acc_v[step % 3, peer] + pr_r[step, peer].astype(F32)
        if order[step] == 0:
            cols = pl.ds(pl.multiple_of(peer * feats, feats), feats)
            term = term + shared_v[:, cols]
            if square:
                term = term + rz_r[peer].astype(F32)
        return term

    def cross(step):
        arrived(pr_r.at[step], pr_recv.at[step])
        if direct(step):
            for b in range(n_tp):
                rs_s[step, b] = block_of(step, b).astype(BF16)
            send(rs_s.at[step], rz_r, rz_send, rz_recv, {"sp": layers[1] * CORES + core})
            return
        if square and order[step] == 0:
            arrived(rz_r, rz_recv)
        if square:
            rs_s[step, 2] = block_of(step, peers[2]).astype(BF16)
            for b in range(2):
                part = pl.ds(b * half, half)
                send(rs_s.at[step, 2, part], rd_r.at[step, part], rs_send.at[step, 2 + b],
                     rs_recv.at[step, 2 + b], {"tp": peers[b]})
        rs_s[step, n_tp - 1] = block_of(step, tp).astype(BF16)

    def spread(step):
        if direct(step):
            return
        if square:
            for b in range(2):
                part = pl.ds(b * half, half)
                arrived(rd_r.at[step, part], rs_recv.at[step, 2 + b])
        for b, peer in enumerate(near):
            term = block_of(step, peer)
            if square:
                part = slice((1 - b) * half, (2 - b) * half)
                extra = rd_r[step, part, :].astype(F32)
                fixed = term[b * half:(b + 1) * half]
                joined = [fixed, term[part] + extra]
                term = jnp.concatenate(joined if b == 0 else joined[::-1], axis=0)
            rs_s[step, b] = term.astype(BF16)
            send(rs_s.at[step, b], rs_r.at[step, b], rs_send.at[step, b],
                 rs_recv.at[step, b], {"tp": peer})

    def gathered(step):
        if direct(step):
            return
        total = rs_s[step, n_tp - 1].astype(F32)
        for b in range(len(near)):
            arrived(rs_r.at[step, b], rs_recv.at[step, b])
            total = total + rs_r[step, b].astype(F32)
        d = order[step]
        if d == 0:
            totals[0] = total
        else:
            zr_s[d] = total.astype(BF16)
            send(zr_s.at[d], zr_r.at[d], zr_send.at[d], zr_recv.at[d],
                 {"sp": layers[d] * CORES + core})

    for step in range(n_z + 2):
        if step < n_z:
            multiply(step)
            if step + 2 < n_z:
                widen(step + 2)
        for lag, stage in enumerate((cross, spread, gathered)):
            if 0 <= step - lag < n_z:
                stage(step - lag)

    result = hidden_v[...] + totals[0]
    for d in range(2 if square else 1, n_z):
        arrived(zr_r.at[d], zr_recv.at[d])
        result = result + zr_r[d].astype(F32)
    out[...] = result.T.astype(BF16)
    for copy in pending:
        copy.wait_send()


def local(n_sp, n_tp, *args):
    (stream, values_in, in_gate, out_gate, documents, conv_taps, head_gain, mix_weight,
     norm_gain, routes, route_weight, expert_gate, expert_up, expert_down,
     shared_gate, shared_up, shared_down) = args
    feats, pos = stream.shape
    chans = values_in.shape[0]
    width = feats * n_tp
    hid = expert_gate.shape[2]
    n_z = n_sp // CORES
    meta_rows = -(-(n_sp + 1) // SUB) * SUB
    vmem = pl.BlockSpec(memory_space=pltpu.VMEM)
    anywhere = pl.BlockSpec(memory_space=pl.ANY)
    dma = pltpu.SemaphoreType.DMA
    scratch = [
        pltpu.VMEM((chans, width), BF16),
        pltpu.VMEM((width, hid), BF16),
        pltpu.VMEM((width, hid), BF16),
        pltpu.VMEM((width, hid), BF16),
        pltpu.VMEM((width, hid), BF16),
        pltpu.VMEM((hid, width), BF16),
        pltpu.VMEM((n_tp, hid, feats), BF16),
        pltpu.VMEM((SUB, chans), F32),
        pltpu.VMEM((pos, chans), F32),
        pltpu.VMEM((1, pos), jnp.int32),
        pltpu.VMEM((n_tp, pos, feats), BF16),
        pltpu.VMEM((n_tp, pos, feats), BF16),
        pltpu.VMEM((pos, feats), F32),
        pltpu.VMEM((n_sp, n_tp, pos, feats), BF16),
        pltpu.VMEM((SUB, pos), F32),
        pltpu.VMEM((n_tp, SUB, pos), F32),
        pltpu.VMEM((n_sp, meta_rows, pos), F32),
        pltpu.VMEM((n_z, CORES * pos, hid), BF16),
        pltpu.VMEM((pos, width), F32),
        pltpu.VMEM((3, n_tp, pos, feats), F32),
        pltpu.VMEM((n_z, n_tp, pos, feats), BF16),
        pltpu.VMEM((n_z, n_tp, pos, feats), BF16),
        pltpu.VMEM((n_z, n_tp, pos, feats), BF16),
        pltpu.VMEM((n_z, n_tp, pos, feats), BF16),
        pltpu.VMEM((n_z if n_tp == 4 else 1, pos, feats), BF16),
        pltpu.VMEM((n_tp if n_tp == 4 else 1, pos, feats), BF16),
        pltpu.VMEM((n_z, pos, feats), BF16),
        pltpu.VMEM((n_z, pos, feats), BF16),
        dma((6,)), dma,
        dma((2,)), dma((2,)),
        dma((n_tp,)), dma((n_tp,)),
        dma((n_tp,)), dma((n_tp,)),
        dma((n_sp,)), dma((n_sp,)),
        dma((n_sp, n_tp)),
        dma((n_z, n_tp)), dma((n_z,)), dma((n_z,)), dma((n_tp,)), dma((n_z, n_tp)),
        dma((n_tp, CHUNKS)), dma((n_tp, CHUNKS)),
        dma((n_z,)), dma((n_z,)),
        dma((n_z, n_tp)), dma((n_z, n_tp)),
        dma((n_z,)), dma((n_z,)),
        dma, dma,
    ]
    return pl.pallas_call(
        functools.partial(kernel, n_sp, n_tp),
        out_shape=jax.ShapeDtypeStruct((feats, pos), BF16),
        in_specs=[vmem] * 7 + [anywhere] + [vmem] * 3 + [anywhere] * 6,
        out_specs=vmem,
        scratch_shapes=scratch,
        compiler_params=pltpu.CompilerParams(
            collective_id=0, has_side_effects=True, vmem_limit_bytes=64 * 1024 * 1024 - 65536
        ),
    )(
        stream, values_in, in_gate, out_gate, documents.reshape(1, pos), conv_taps,
        head_gain.reshape(1, chans), mix_weight, norm_gain.reshape(1, feats), routes.T,
        route_weight.T, expert_gate, expert_up, expert_down, shared_gate, shared_up, shared_down,
    )


def solution(mesh):
    in_specs = (
        P("tp", "sp"),
        P("tp", "sp"),
        P("tp", "sp"),
        P("tp", "sp"),
        P("sp"),
        P(None, "tp"),
        P("tp"),
        P("tp", None),
        P("tp"),
        P("sp", None),
        P("sp", None),
        P("sp", None, "tp"),
        P("sp", None, "tp"),
        P("sp", None, "tp"),
        P(None, "tp"),
        P(None, "tp"),
        P("tp", None),
    )
    body = functools.partial(local, mesh.shape["sp"], mesh.shape["tp"])
    return jax.shard_map(
        body, mesh=mesh, in_specs=in_specs, out_specs=P("tp", "sp"), check_vma=False
    )
```

```python
import functools

import jax
import jax.numpy as jnp
from jax import lax
from jax.experimental import pallas as pl
from jax.experimental.pallas import tpu as pltpu
from jax.sharding import PartitionSpec as P

HEAD = 64
CORES = 2
CHUNKS = 8
SUB = 8
PLAN = (1, 1, 1, 5, 0)
ALONG_Z = (1, 2)
epsilon = 1e-06
MESH = pl.DeviceIdType.MESH
F32 = jnp.float32
BF16 = jnp.bfloat16


def flipped(index, mask):
    bit = 1
    out = index
    while bit <= mask:
        if mask & bit:
            out = out + bit - 2 * bit * lax.rem(lax.div(index, bit), 2)
        bit *= 2
    return out


def dot(left, right):
    return jnp.dot(left, right, preferred_element_type=F32)


def silu(value):
    return value / (1.0 + jnp.exp(-value))


def column_of(row, width):
    return jnp.broadcast_to(row, (width, row.shape[1])).T


def kernel(
    n_sp, n_tp,
    stream, values_in, in_gate, out_gate, documents, conv_taps, head_gain, mix_weight,
    norm_gain, routes, route_weight, expert_gate, expert_up, expert_down,
    shared_gate, shared_up, shared_down,
    out,
    mix_w, gate_w, up_w, sgate_w, sup_w, sdown_w, down_w,
    tail_s, prev_r, prev_docs, mix_s, mix_r, hidden_v, x_all, ss_s, ss_r, meta_r,
    mid_v, shared_v, acc_v, pr_s, pr_r, rs_s, rs_r, rd_r, rz_r, zr_s, zr_r,
    load_sem, local_sem, halo_send, halo_recv, mix_send, mix_recv, ss_send, ss_recv,
    meta_send, meta_recv, x_recv, xs_tp, xs_z, xs_d, xs_n, xs_p, wd_send, wd_recv,
    pr_send, pr_recv, rs_send, rs_recv, zr_send, zr_recv, rz_send, rz_recv,
):
    sp = lax.axis_index("sp")
    tp = lax.axis_index("tp")
    z = lax.div(sp, CORES)
    core = lax.rem(sp, CORES)
    n_z = n_sp // CORES
    feats, pos = stream.shape
    chans = values_in.shape[0]
    width = feats * n_tp
    hid = gate_w.shape[1]
    partner = {"sp": z * CORES + 1 - core}
    peers = [flipped(tp, d) for d in range(1, n_tp)]
    square = n_tp == 4 and n_z > 1
    near = peers[:2] if square else peers
    along_z = [d for d in ALONG_Z if d < n_z] if square else []
    layers = [flipped(z, d) for d in range(n_z)]
    pending = []

    def send(src, dst, ssem, rsem, device):
        copy = pltpu.make_async_remote_copy(
            src_ref=src, dst_ref=dst, send_sem=ssem, recv_sem=rsem,
            device_id=device, device_id_type=MESH,
        )
        copy.start()
        pending.append(copy)

    def arrived(dst, rsem):
        pltpu.make_async_remote_copy(
            src_ref=dst, dst_ref=dst, send_sem=rsem, recv_sem=rsem,
            device_id=partner, device_id_type=MESH,
        ).wait_recv()

    loads = [
        pltpu.make_async_copy(src, dst, load_sem.at[i])
        for i, (src, dst) in enumerate([
            (mix_weight, mix_w), (shared_gate, sgate_w), (shared_up, sup_w),
            (shared_down, sdown_w), (expert_gate.at[0], gate_w), (expert_up.at[0], up_w),
        ])
    ]
    loads[0].start()

    barrier = pltpu.get_barrier_semaphore()
    for peer in peers:
        pl.semaphore_signal(barrier, inc=1, device_id={"tp": peer}, device_id_type=MESH)
    for d in range(1, n_sp):
        pl.semaphore_signal(
            barrier, inc=1, device_id={"sp": lax.rem(sp + d, n_sp)}, device_id_type=MESH
        )
    pl.semaphore_wait(barrier, n_tp - 1 + n_sp - 1)

    product = values_in[...].astype(F32) * in_gate[...].astype(F32)
    tail_s[...] = product.T[pos - SUB:, :]
    after = {"sp": lax.rem(sp + 1, n_sp)}
    send(tail_s, prev_r.at[pl.ds(pos - SUB, SUB)], halo_send.at[0], halo_recv.at[0], after)
    send(documents, prev_docs, halo_send.at[1], halo_recv.at[1], after)

    rows = hid // CHUNKS

    sent_chunks = []

    def send_chunks(stage):
        for _ in range(PLAN[stage]):
            send_down(len(sent_chunks))
            sent_chunks.append(stage)

    def send_down(chunk):
        for d, peer in enumerate(peers):
            start = pl.multiple_of(peer * hid + chunk * rows, rows)
            send(
                expert_down.at[0, pl.ds(start, rows), :],
                down_w.at[tp, pl.ds(chunk * rows, rows), :],
                wd_send.at[d, chunk], wd_recv.at[tp, chunk], {"tp": peer},
            )

    send_chunks(0)
    own_down = pltpu.make_async_copy(
        expert_down.at[0, pl.ds(pl.multiple_of(tp * hid, hid), hid), :], down_w.at[tp], local_sem
    )
    for load in loads[1:]:
        load.start()
    own_down.start()

    named = routes[...]
    weights = route_weight[...]
    meta_rows = meta_r.shape[1]
    at_row = lax.broadcasted_iota(jnp.int32, (meta_rows, pos), 0)
    table = jnp.zeros((meta_rows, pos), F32)
    for k in range(routes.shape[0]):
        table = table + jnp.where(at_row == named[k:k + 1, :], weights[k:k + 1, :], 0.0)
    taps = [column_of(conv_taps[j:j + 1, :], pos) for j in range(3)]
    stream_t = stream[...].astype(F32).T

    prev_r[: pos - SUB, :] = jnp.zeros((pos - SUB, chans), F32)
    arrived(prev_r.at[pl.ds(pos - SUB, SUB)], halo_recv.at[0])
    arrived(prev_docs, halo_recv.at[1])
    before = prev_r[...].T
    docs = documents[...]
    docs_before = jnp.where(sp > 0, prev_docs[...], -1)
    lane_c = lax.broadcasted_iota(jnp.int32, (chans, pos), 1)
    lane_1 = lax.broadcasted_iota(jnp.int32, (1, pos), 1)
    convolved = taps[2] * product
    for shift in (1, 2):
        moved = jnp.where(lane_c < shift, pltpu.roll(before, shift, 1), pltpu.roll(product, shift, 1))
        ids = jnp.where(lane_1 < shift, pltpu.roll(docs_before, shift, 1), pltpu.roll(docs, shift, 1))
        convolved = convolved + jnp.where(ids == docs, taps[2 - shift] * moved, 0.0)
    mixed = out_gate[...].astype(F32) * convolved
    heads = mixed.reshape(chans // HEAD, HEAD, pos)
    heads = heads * lax.rsqrt(jnp.mean(heads * heads, axis=1, keepdims=True) + epsilon)
    heads_t = (heads.reshape(chans, pos).T * head_gain[...]).astype(BF16)

    loads[0].wait()
    for b, peer in enumerate(peers + [tp]):
        cols = pl.ds(pl.multiple_of(peer * feats, feats), feats)
        mix_s[b] = dot(heads_t, mix_w[:, cols]).astype(BF16)
        if b < n_tp - 1:
            send(mix_s.at[b], mix_r.at[b], mix_send.at[b], mix_recv.at[b], {"tp": peer})
    send_chunks(1)

    hidden = stream_t + mix_s[n_tp - 1].astype(F32)
    for b in range(n_tp - 1):
        arrived(mix_r.at[b], mix_recv.at[b])
        hidden = hidden + mix_r[b].astype(F32)
    hidden_v[...] = hidden
    x_all[sp, tp] = (hidden * norm_gain[...]).astype(BF16)
    own = x_all.at[sp, tp]
    for d in range(1, n_z):
        send(own, own, xs_z.at[d], x_recv.at[sp, tp], {"sp": layers[d] * CORES + core})
    for b, peer in enumerate(peers):
        send(own, own, xs_tp.at[0, b], x_recv.at[sp, tp], {"tp": peer})
    send(own, own, xs_p.at[0, 0], x_recv.at[sp, tp], partner)

    squares = jnp.sum(hidden * hidden, axis=1, keepdims=True)
    row = jnp.broadcast_to(squares, (pos, pos)).T[:SUB]
    ss_s[...] = row
    for b, peer in enumerate(peers):
        send(ss_s, ss_r.at[b], ss_send.at[b], ss_recv.at[b], {"tp": peer})
    send_chunks(2)
    for b in range(n_tp - 1):
        arrived(ss_r.at[b], ss_recv.at[b])
        row = row + ss_r[b]
    scale = lax.rsqrt(row[:1] / width + epsilon)
    meta_r[sp] = jnp.where(at_row == meta_rows - 1, scale, table)
    for d in range(1, n_sp):
        send(meta_r.at[sp], meta_r.at[sp], meta_send.at[d], meta_recv.at[sp],
             {"sp": lax.rem(sp + d, n_sp)})

    def to_partner(slot, b, group):
        block = x_all.at[group, peers[b]]
        arrived(block, x_recv.at[group, peers[b]])
        send(block, block, xs_p.at[slot, b + 1], x_recv.at[group, peers[b]], partner)

    def from_layer(d):
        group = layers[d] * CORES + core
        block = x_all.at[group, tp]
        arrived(block, x_recv.at[group, tp])
        for b, peer in enumerate([] if square and d == 1 else (near if d in along_z else peers)):
            send(block, block, xs_tp.at[d, b], x_recv.at[group, tp], {"tp": peer})
        send(block, block, xs_p.at[d, 0], x_recv.at[group, tp], partner)

    for b in range(n_tp - 1):
        to_partner(0, b, sp)
        if square and b < 2:
            block = x_all.at[sp, peers[b]]
            send(block, block, xs_n.at[b], x_recv.at[sp, peers[b]],
                 {"sp": layers[1] * CORES + core})
    if square:
        block = x_all.at[sp, peers[2]]
        for d in along_z:
            send(block, block, xs_d.at[d], x_recv.at[sp, peers[2]],
                 {"sp": layers[d] * CORES + core})
    from_layer(1)
    send_chunks(3)

    loads[1].wait()
    loads[2].wait()
    scale_own = column_of(scale, pos)[:, :1]
    gate = jnp.zeros((pos, hid), F32)
    upward = jnp.zeros((pos, hid), F32)
    for b in range(n_tp):
        block = x_all[sp, b]
        gate = gate + dot(block, sgate_w[b * feats:(b + 1) * feats, :])
        upward = upward + dot(block, sup_w[b * feats:(b + 1) * feats, :])
    shared_mid = (silu(gate * scale_own) * (upward * scale_own)).astype(BF16)
    loads[3].wait()
    shared_v[...] = dot(shared_mid, sdown_w[...])

    for d in range(2, n_z):
        from_layer(d)
    send_chunks(4)

    loads[4].wait()
    loads[5].wait()
    def widen(d):
        layer = layers[d]
        mine = layer * CORES + core
        other = layer * CORES + 1 - core
        if d > 0:
            for b in range(n_tp - 1):
                to_partner(d, b, mine)
            arrived(meta_r.at[mine], meta_recv.at[mine])
        arrived(meta_r.at[other], meta_recv.at[other])
        for b in range(n_tp):
            arrived(x_all.at[other, b], x_recv.at[other, b])
        gate = jnp.zeros((CORES * pos, hid), F32)
        upward = jnp.zeros((CORES * pos, hid), F32)
        for b in range(n_tp):
            block = x_all[pl.ds(layer * CORES, CORES), b].reshape(CORES * pos, feats)
            gate = gate + dot(block, gate_w[b * feats:(b + 1) * feats, :])
            upward = upward + dot(block, up_w[b * feats:(b + 1) * feats, :])
        scales = jnp.concatenate([
            column_of(meta_r[layer * CORES + i, meta_rows - 1:, :], pos)[:, :1]
            for i in range(CORES)
        ], axis=0)
        mid_v[layer] = (silu(gate * scales) * (upward * scales)).astype(BF16)

    widen(0)
    if n_z > 1:
        widen(1)
    own_down.wait()
    for peer in peers:
        for chunk in range(CHUNKS):
            arrived(down_w.at[peer, pl.ds(chunk * rows, rows), :], wd_recv.at[peer, chunk])

    order = list(range(1, n_z)) + [0]
    half = pos // 2

    def direct(step):
        return square and order[step] == 1

    totals = {}

    def multiply(step):
        layer = layers[order[step]]
        weight = jnp.concatenate([
            column_of(meta_r[layer * CORES + i, pl.ds(sp, 1), :], pos)[:, :1]
            for i in range(CORES)
        ], axis=0)
        middle = mid_v[layer]
        for b in range(n_tp):
            term = dot(middle, down_w[b]) * weight
            lower, upper = term[:pos], term[pos:]
            pr_s[step, b] = jnp.where(core == 0, upper, lower).astype(BF16)
            acc_v[step % 3, b] = jnp.where(core == 0, lower, upper)
        send(pr_s.at[step], pr_r.at[step], pr_send.at[step], pr_recv.at[step], partner)

    def block_of(step, peer):
        term = acc_v[step % 3, peer] + pr_r[step, peer].astype(F32)
        if order[step] == 0:
            cols = pl.ds(pl.multiple_of(peer * feats, feats), feats)
            term = term + shared_v[:, cols]
            if square:
                term = term + rz_r[peer].astype(F32)
        return term

    def cross(step):
        arrived(pr_r.at[step], pr_recv.at[step])
        if direct(step):
            for b in range(n_tp):
                rs_s[step, b] = block_of(step, b).astype(BF16)
            send(rs_s.at[step], rz_r, rz_send, rz_recv, {"sp": layers[1] * CORES + core})
            return
        if square and order[step] == 0:
            arrived(rz_r, rz_recv)
        if square:
            rs_s[step, 2] = block_of(step, peers[2]).astype(BF16)
            for b in range(2):
                part = pl.ds(b * half, half)
                send(rs_s.at[step, 2, part], rd_r.at[step, part], rs_send.at[step, 2 + b],
                     rs_recv.at[step, 2 + b], {"tp": peers[b]})
        rs_s[step, n_tp - 1] = block_of(step, tp).astype(BF16)

    def spread(step):
        if direct(step):
            return
        if square:
            for b in range(2):
                part = pl.ds(b * half, half)
                arrived(rd_r.at[step, part], rs_recv.at[step, 2 + b])
        for b, peer in enumerate(near):
            term = block_of(step, peer)
            if square:
                part = slice((1 - b) * half, (2 - b) * half)
                extra = rd_r[step, part, :].astype(F32)
                fixed = term[b * half:(b + 1) * half]
                joined = [fixed, term[part] + extra]
                term = jnp.concatenate(joined if b == 0 else joined[::-1], axis=0)
            rs_s[step, b] = term.astype(BF16)
            send(rs_s.at[step, b], rs_r.at[step, b], rs_send.at[step, b],
                 rs_recv.at[step, b], {"tp": peer})

    def gathered(step):
        if direct(step):
            return
        total = rs_s[step, n_tp - 1].astype(F32)
        for b in range(len(near)):
            arrived(rs_r.at[step, b], rs_recv.at[step, b])
            total = total + rs_r[step, b].astype(F32)
        d = order[step]
        if d == 0:
            totals[0] = total
        else:
            zr_s[d] = total.astype(BF16)
            send(zr_s.at[d], zr_r.at[d], zr_send.at[d], zr_recv.at[d],
                 {"sp": layers[d] * CORES + core})

    for step in range(n_z + 2):
        if step < n_z:
            multiply(step)
            if step + 2 < n_z:
                widen(step + 2)
        for lag, stage in enumerate((cross, spread, gathered)):
            if 0 <= step - lag < n_z:
                stage(step - lag)

    result = hidden_v[...] + totals[0]
    for d in range(2 if square else 1, n_z):
        arrived(zr_r.at[d], zr_recv.at[d])
        result = result + zr_r[d].astype(F32)
    out[...] = result.T.astype(BF16)
    for copy in pending:
        copy.wait_send()


def local(n_sp, n_tp, *args):
    (stream, values_in, in_gate, out_gate, documents, conv_taps, head_gain, mix_weight,
     norm_gain, routes, route_weight, expert_gate, expert_up, expert_down,
     shared_gate, shared_up, shared_down) = args
    feats, pos = stream.shape
    chans = values_in.shape[0]
    width = feats * n_tp
    hid = expert_gate.shape[2]
    n_z = n_sp // CORES
    meta_rows = -(-(n_sp + 1) // SUB) * SUB
    vmem = pl.BlockSpec(memory_space=pltpu.VMEM)
    anywhere = pl.BlockSpec(memory_space=pl.ANY)
    dma = pltpu.SemaphoreType.DMA
    scratch = [
        pltpu.VMEM((chans, width), BF16),
        pltpu.VMEM((width, hid), BF16),
        pltpu.VMEM((width, hid), BF16),
        pltpu.VMEM((width, hid), BF16),
        pltpu.VMEM((width, hid), BF16),
        pltpu.VMEM((hid, width), BF16),
        pltpu.VMEM((n_tp, hid, feats), BF16),
        pltpu.VMEM((SUB, chans), F32),
        pltpu.VMEM((pos, chans), F32),
        pltpu.VMEM((1, pos), jnp.int32),
        pltpu.VMEM((n_tp, pos, feats), BF16),
        pltpu.VMEM((n_tp, pos, feats), BF16),
        pltpu.VMEM((pos, feats), F32),
        pltpu.VMEM((n_sp, n_tp, pos, feats), BF16),
        pltpu.VMEM((SUB, pos), F32),
        pltpu.VMEM((n_tp, SUB, pos), F32),
        pltpu.VMEM((n_sp, meta_rows, pos), F32),
        pltpu.VMEM((n_z, CORES * pos, hid), BF16),
        pltpu.VMEM((pos, width), F32),
        pltpu.VMEM((3, n_tp, pos, feats), F32),
        pltpu.VMEM((n_z, n_tp, pos, feats), BF16),
        pltpu.VMEM((n_z, n_tp, pos, feats), BF16),
        pltpu.VMEM((n_z, n_tp, pos, feats), BF16),
        pltpu.VMEM((n_z, n_tp, pos, feats), BF16),
        pltpu.VMEM((n_z if n_tp == 4 else 1, pos, feats), BF16),
        pltpu.VMEM((n_tp if n_tp == 4 else 1, pos, feats), BF16),
        pltpu.VMEM((n_z, pos, feats), BF16),
        pltpu.VMEM((n_z, pos, feats), BF16),
        dma((6,)), dma,
        dma((2,)), dma((2,)),
        dma((n_tp,)), dma((n_tp,)),
        dma((n_tp,)), dma((n_tp,)),
        dma((n_sp,)), dma((n_sp,)),
        dma((n_sp, n_tp)),
        dma((n_z, n_tp)), dma((n_z,)), dma((n_z,)), dma((n_tp,)), dma((n_z, n_tp)),
        dma((n_tp, CHUNKS)), dma((n_tp, CHUNKS)),
        dma((n_z,)), dma((n_z,)),
        dma((n_z, n_tp)), dma((n_z, n_tp)),
        dma((n_z,)), dma((n_z,)),
        dma, dma,
    ]
    return pl.pallas_call(
        functools.partial(kernel, n_sp, n_tp),
        out_shape=jax.ShapeDtypeStruct((feats, pos), BF16),
        in_specs=[vmem] * 7 + [anywhere] + [vmem] * 3 + [anywhere] * 6,
        out_specs=vmem,
        scratch_shapes=scratch,
        compiler_params=pltpu.CompilerParams(
            collective_id=0, has_side_effects=True, vmem_limit_bytes=64 * 1024 * 1024 - 65536
        ),
    )(
        stream, values_in, in_gate, out_gate, documents.reshape(1, pos), conv_taps,
        head_gain.reshape(1, chans), mix_weight, norm_gain.reshape(1, feats), routes.T,
        route_weight.T, expert_gate, expert_up, expert_down, shared_gate, shared_up, shared_down,
    )


def solution(mesh):
    in_specs = (
        P("tp", "sp"),
        P("tp", "sp"),
        P("tp", "sp"),
        P("tp", "sp"),
        P("sp"),
        P(None, "tp"),
        P("tp"),
        P("tp", None),
        P("tp"),
        P("sp", None),
        P("sp", None),
        P("sp", None, "tp"),
        P("sp", None, "tp"),
        P("sp", None, "tp"),
        P(None, "tp"),
        P(None, "tp"),
        P("tp", None),
    )
    body = functools.partial(local, mesh.shape["sp"], mesh.shape["tp"])
    return jax.shard_map(
        body, mesh=mesh, in_specs=in_specs, out_specs=P("tp", "sp"), check_vma=False
    )
```
